256 devices in a mesh: ep: 16 (over y, x), tp: 16 (over z, core).
Axes of the slice: x: 4, y: 4, z: 8, core: 2. Of those that a mesh axis runs over, the one named last changes fastest.
Arguments:
- tokens: bfloat16 [3072, 2048], P('ep'), may hold values from -6 to 6
- cotangent: bfloat16 [3072, 2048], P('ep'), may hold values from -6 to 6
- routing: int32 [3072, 2], P('ep'), may hold values from 0 to 15, all different within a row; in each aligned block of 192 rows (0 to 191, 192 to 383, ...) at most 48 rows name the same one
- gate_weights: bfloat16 [3072, 2], P('ep'), may hold values from 0.19921875 to 1
- gate_proj: bfloat16 [16, 2048, 7168], P('ep', None, 'tp'), may hold values from -0.125 to 0.125
- up_proj: bfloat16 [16, 2048, 7168], P('ep', None, 'tp'), may hold values from -0.125 to 0.125
- down_proj: bfloat16 [16, 7168, 2048], P('ep', 'tp'), may hold values from -0.0625 to 0.0625
Outputs:
- grad_tokens: bfloat16 [3072, 2048], P('ep', 'tp')
- grad_gates: float32 [3072, 2], P('ep')
- grad_gate_proj: bfloat16 [16, 2048, 7168], P('ep', None, 'tp')
- grad_up_proj: bfloat16 [16, 2048, 7168], P('ep', None, 'tp')
- grad_down_proj: bfloat16 [16, 7168, 2048], P('ep', 'tp')
The draws below stay inside these ranges and needn't reach their ends.
Inputs may be any that keep to these rules, and one draw needn't show every extreme that they name: `routing`: each row names 2 different experts. Within each aligned block of 192 rows no expert is named by more than 48 rows, and in every draw some expert is named by exactly 48 rows of some block.
All inputs are finite; a program needn't handle non-finite values.
Results may differ from the reference program's by a relative error of at most 0.019.
Values may be sent and summed in bfloat16 or wider, within the bound.
No kernel may reach another device: no remote copies, remote signals or barrier semaphores. Data moves between devices by JAX's collectives and lax.ppermute only.
A program may use at most 128 MiB of HBM per device.

```python
import math
import jax
import jax.numpy as jnp
import numpy as np
from jax import lax

D = 2048
FF = 7168
TOP_K = 2
TOK_DEV = 192
EXPERTS = 16
CAP = 48
TOKENS = 3072
N_EP = 16


def block_scale(stream_key, shape, shards, least, high):
    def one(axis_at, shards_of):
        steps = jax.random.uniform(jax.random.fold_in(jax.random.fold_in(stream_key, 6), axis_at), (shards_of,), jnp.float32, least / len(shards), high / len(shards))
        return jnp.repeat(jnp.exp(steps), shape[axis_at] // shards_of).reshape((-1,) + (1,) * (len(shape) - axis_at - 1))

    level = one(*shards[0])
    for cut in shards[1:]:
        level = level * one(*cut)
    return level


def assign_block(rng, own, number, rows, count, top, limit, slope):
    sequence = jax.random.permutation(rng, count)
    crowded, usual = load_shares(count, rows * top, limit, slope, True), load_shares(count, rows * top, limit, slope, False)
    places = jnp.arange(count)

    def named(sizes, turn):
        used = int((sizes > 0).sum())
        fixed = max(1, used // 4)
        shifted = fixed + (places - fixed + turn * (used - fixed)) % max(1, count - fixed)
        return jnp.zeros((count,), jnp.int32).at[sequence[jnp.where(places < fixed, places, shifted)]].set(jnp.asarray(sizes, jnp.int32))

    sizes = jnp.where(number % 4 == 0, named(crowded, number // 4), named(usual, number - number // 4 - 1))
    mixed = jax.random.permutation(jax.random.fold_in(own, 3), count)
    donor, taker = mixed[0:count // 2 * 2:2], mixed[1:count // 2 * 2:2]
    room = jnp.minimum(sizes[donor] - 1, limit - sizes[taker]) // 2
    room = jnp.where((donor == sequence[0]) | (taker == sequence[0]) | (sizes[taker] == 0), 0, jnp.maximum(room, 0))
    shifted = jax.random.randint(jax.random.fold_in(own, 4), (count // 2,), 0, 1 << 20) % (room + 1)
    sizes = sizes.at[donor].add(-shifted).at[taker].add(shifted)
    items = jnp.searchsorted(jnp.cumsum(sizes), jnp.arange(rows * top), side="right").astype(jnp.int32)
    grid = items.reshape(top, rows).T
    grid = grid[jax.random.permutation(jax.random.fold_in(own, 1), rows)]
    turn = jax.random.randint(jax.random.fold_in(own, 2), (rows, 1), 0, top)
    return jnp.take_along_axis(grid, (jnp.arange(top)[None, :] + turn) % top, axis=1)


def load_shares(number_of, total, most, lean, full):
    portions = [(1 << 20) // math.isqrt(rank ** lean) + 1 for rank in range(1, number_of + 1)]
    largest = most if full else min(most, max(-(-total // number_of), total * portions[0] // sum(portions)))
    least = 1 if total - largest >= number_of - 1 else 0
    counts, surplus = [largest] + [least] * (number_of - 1), total - largest - least * (number_of - 1)
    while surplus > 0:
        free = [i for i in range(1, number_of) if counts[i] < largest] or [i for i in range(1, number_of) if counts[i] < most]
        pool, budget = sum([portions[i] for i in free]), surplus
        for i in free:
            addition = min(most - counts[i], max(1, budget * portions[i] // pool), surplus)
            counts[i] = counts[i] + addition
            surplus = surplus - addition
    return np.array(counts)


def normal_values(rng, extent, deviation, reach, cuts=(), kind=jnp.bfloat16):
    drawn = jax.random.normal(rng, extent, jnp.float32) * deviation
    if len(cuts) > 0:
        drawn = block_scale(rng, extent, cuts, -0.22, 0.18) * drawn
    return jnp.clip(drawn, min=-reach, max=reach).astype(kind)


def setup_inputs(seed: int = 0) -> dict:
    streams_of = jax.random.split(jax.random.key(seed), 8)
    tokens = normal_values(streams_of[0], (TOKENS, D), 1.0, 6.0, ((0, 16),))
    cotangent = normal_values(streams_of[1], (TOKENS, D), 1.0, 6.0, ((0, 16),))
    routing_keys = jax.random.split(jax.random.fold_in(streams_of[2], 1), TOKENS // TOK_DEV)
    routing_turns = jax.random.permutation(jax.random.fold_in(streams_of[2], 3), TOKENS // TOK_DEV)
    routing = jax.vmap(lambda own, number: assign_block(jax.random.fold_in(streams_of[2], 2), own, number, TOK_DEV, EXPERTS, TOP_K, CAP, 1))(routing_keys, routing_turns).reshape((TOKENS, TOP_K))
    gate_weights = jnp.clip(0.19921875 + 0.80078125 * jax.random.uniform(streams_of[3], (TOKENS, TOP_K), jnp.float32) ** block_scale(streams_of[3], (TOKENS, TOP_K), ((0, 16),), -0.2, 0.2), 0.19921875, 1.0).astype(jnp.bfloat16)
    gate_proj = normal_values(streams_of[4], (EXPERTS, D, FF), D ** -0.5, 0.125, ((0, 16), (2, 16)))
    up_proj = normal_values(streams_of[5], (EXPERTS, D, FF), D ** -0.5, 0.125, ((0, 16), (2, 16)))
    down_proj = normal_values(streams_of[6], (EXPERTS, FF, D), FF ** -0.5, 0.0625, ((0, 16), (1, 16)))
    return {"tokens": tokens, "cotangent": cotangent, "routing": routing, "gate_weights": gate_weights, "gate_proj": gate_proj, "up_proj": up_proj, "down_proj": down_proj}


def expert_backward(in_rows, cot_rows, gate_col, w_gate, w_up, w_down):
    gate_pre = jnp.dot(in_rows, w_gate, preferred_element_type=jnp.float32)
    up_value = jnp.dot(in_rows, w_up, preferred_element_type=jnp.float32)
    sigmoid_val = jax.nn.sigmoid(gate_pre)
    active = gate_pre * sigmoid_val
    hidden = (active * up_value).astype(jnp.bfloat16)
    contract_cols = (((1,), (1,)), ((), ()))
    contract_rows = (((0,), (0,)), ((), ()))
    back_hidden = lax.dot_general(cot_rows, w_down, contract_cols, preferred_element_type=jnp.float32)
    gate_part = jnp.sum(hidden.astype(jnp.float32) * back_hidden, axis=1)
    scaled_back = gate_col * back_hidden
    grad_pre = (scaled_back * up_value * sigmoid_val * (1.0 + gate_pre * (1.0 - sigmoid_val))).astype(jnp.bfloat16)
    grad_upval = (scaled_back * active).astype(jnp.bfloat16)
    scaled_cot = (gate_col * cot_rows.astype(jnp.float32)).astype(jnp.bfloat16)
    grad_down = lax.dot_general(hidden, scaled_cot, contract_rows, preferred_element_type=jnp.float32).astype(jnp.bfloat16)
    grad_gate = lax.dot_general(in_rows, grad_pre, contract_rows, preferred_element_type=jnp.float32).astype(jnp.bfloat16)
    grad_upw = lax.dot_general(in_rows, grad_upval, contract_rows, preferred_element_type=jnp.float32).astype(jnp.bfloat16)
    grad_in = lax.dot_general(grad_pre, w_gate, contract_cols, preferred_element_type=jnp.float32)
    grad_in = grad_in + lax.dot_general(grad_upval, w_up, contract_cols, preferred_element_type=jnp.float32)
    return grad_in, gate_part, grad_gate, grad_upw, grad_down


def reference(tokens, cotangent, routing, gate_weights, gate_proj, up_proj, down_proj):
    block_len = TOK_DEV * TOP_K
    flat_routes = routing.reshape(N_EP, block_len).astype(jnp.int32)
    onehot = (flat_routes[:, :, None] == jnp.arange(EXPERTS, dtype=jnp.int32)[None, None, :]).astype(jnp.int32)
    position = (jnp.sum(jnp.cumsum(onehot, axis=1) * onehot, axis=2) - 1).astype(jnp.int32)
    source = jnp.broadcast_to(jnp.arange(N_EP, dtype=jnp.int32)[:, None], (N_EP, block_len))
    global_index = source * block_len + jnp.arange(block_len, dtype=jnp.int32)[None, :]
    slot_owner = jnp.full((EXPERTS, N_EP, CAP), -1, jnp.int32).at[flat_routes, source, position].set(global_index)
    slot_owner = slot_owner.reshape(EXPERTS, N_EP * CAP)
    flat_gates = gate_weights.reshape(-1)

    def one_expert(inputs):
        w_gate, w_up, w_down, owner = inputs
        is_used = owner >= 0
        safe_owner = jnp.where(is_used, owner, 0)
        token_index = safe_owner // TOP_K
        in_rows = jnp.where(is_used[:, None], tokens[token_index], jnp.zeros((), jnp.bfloat16))
        cot_rows = jnp.where(is_used[:, None], cotangent[token_index], jnp.zeros((), jnp.bfloat16))
        gate_col = jnp.where(is_used, flat_gates[safe_owner].astype(jnp.float32), 0.0)[:, None]
        return expert_backward(in_rows, cot_rows, gate_col, w_gate, w_up, w_down)

    grad_in, gate_part, grad_gate, grad_upw, grad_down = lax.map(one_expert, (gate_proj, up_proj, down_proj, slot_owner))
    slot_index = (flat_routes * (N_EP * CAP) + source * CAP + position).reshape(-1)
    picked = grad_in.reshape(EXPERTS * N_EP * CAP, D)[slot_index]
    grad_tokens = jnp.sum(picked.reshape(TOKENS, TOP_K, D), axis=1).astype(jnp.bfloat16)
    grad_gates = gate_part.reshape(-1)[slot_index].reshape(TOKENS, TOP_K)
    return grad_tokens, grad_gates, grad_gate, grad_upw, grad_down
```

```python
import functools

import jax
import jax.numpy as jnp
from jax import lax
from jax.experimental import pallas as pl
from jax.experimental.pallas import tpu as pltpu
from jax.sharding import PartitionSpec as P

EP = ("y", "x")
LANES = 128
BF16 = jnp.bfloat16
F32 = jnp.float32
NN = (((1,), (0,)), ((), ()))
NT = (((1,), (1,)), ((), ()))
TN = (((0,), (0,)), ((), ()))
VMEM = pl.BlockSpec(memory_space=pltpu.VMEM)
SMEM = pl.BlockSpec(memory_space=pltpu.SMEM)


def dot(a, b, dims):
    return lax.dot_general(a, b, dims, preferred_element_type=F32)


def call(kernel, out_shape, *args, in_specs=None, flops=0):
    moved = sum(a.size * a.dtype.itemsize for a in (*args, *jax.tree.leaves(out_shape)))
    return pl.pallas_call(
        kernel,
        out_shape=out_shape,
        in_specs=in_specs or [VMEM] * len(args),
        out_specs=jax.tree.map(lambda _: VMEM, out_shape),
        cost_estimate=pl.CostEstimate(flops=flops, bytes_accessed=moved, transcendentals=0),
        compiler_params=pltpu.CompilerParams(vmem_limit_bytes=56 * 1024 * 1024),
    )(*args)


def slots_of(core, routes, experts, half):
    top_k, rows = routes.shape
    expert = lax.broadcasted_iota(jnp.int32, (experts, rows), 0)
    hits = [routes[k : k + 1, :] == expert for k in range(top_k)]
    named = functools.reduce(jnp.logical_or, hits)
    before = lax.broadcasted_iota(jnp.int32, (rows, rows), 0) < lax.broadcasted_iota(
        jnp.int32, (rows, rows), 1
    )
    ones = lambda mask: jnp.where(mask, 1.0, 0.0).astype(BF16)
    count = dot(ones(named), ones(before), NN)
    slots = []
    for k in range(top_k):
        place = jnp.sum(jnp.where(hits[k], count, 0.0), axis=0, keepdims=True).astype(jnp.int32)
        place = place - core * half
        inside = (place >= 0) & (place < half)
        slots.append(jnp.where(inside, routes[k : k + 1, :] * half + place, -1))
    return slots


def masks_of(slots, count):
    row = lax.broadcasted_iota(jnp.int32, (count, slots[0].shape[1]), 0)
    return [row == s for s in slots]


def prepare(experts, half, core_ref, routes_ref, gates_ref, tok_ref, cot_ref, out_ref):
    width = tok_ref.shape[1]
    slots = slots_of(core_ref[0], routes_ref[...], experts, half)
    masks = masks_of(slots, experts * half)
    gates = gates_ref[...].astype(F32)
    pick = jnp.zeros(masks[0].shape, F32)
    weigh = jnp.zeros(masks[0].shape, F32)
    for k, mask in enumerate(masks):
        pick = jnp.where(mask, 1.0, pick)
        weigh = jnp.where(mask, gates[k : k + 1, :], weigh)
    out_ref[:, :width] = dot(pick.astype(BF16), tok_ref[...], NN).astype(BF16)
    out_ref[:, width:] = dot(weigh.astype(BF16), cot_ref[...], NN).astype(BF16)


def expert(x_ref, *refs):
    weights, outs = refs[:6], refs[6:]
    back_ref, hid_ref, pre_ref, up_ref = outs
    width = weights[0].shape[1]
    tok = x_ref[:, :width]
    cot = x_ref[:, width:]
    gate = jnp.zeros((x_ref.shape[0], 1), F32)
    for part in range(2):
        wg, wu, wd = weights[3 * part : 3 * part + 3]
        pre = dot(tok, wg[...], NT)
        up = dot(tok, wu[...], NT)
        back = dot(cot, wd[...], NT)
        sig = jax.nn.sigmoid(pre)
        act = pre * sig
        hidden = (act * up).astype(BF16)
        gate = gate + jnp.sum(hidden.astype(F32) * back, axis=1, keepdims=True)
        hid_ref[part] = hidden
        pre_ref[part] = (back * up * sig * (1.0 + pre * (1.0 - sig))).astype(BF16)
        up_ref[part] = (back * act).astype(BF16)
    total = dot(pre_ref[0], weights[0][...], NN)
    total += dot(up_ref[0], weights[1][...], NN)
    total += dot(pre_ref[1], weights[3][...], NN)
    total += dot(up_ref[1], weights[4][...], NN)
    back_ref[:, :width] = total.astype(BF16)
    back_ref[:, width:] = jnp.broadcast_to(gate, (gate.shape[0], LANES)).astype(BF16)


def weight_grads(part, width, x_ref, hid_ref, pre_ref, up_ref, *refs):
    lefts = (pre_ref, up_ref, hid_ref)
    if len(refs) > 3:
        received, outs = refs[:3], refs[3:]
    else:
        received, outs = (None,) * 3, refs
    for n in range(3):
        right = x_ref[:, width:] if n == 2 else x_ref[:, :width]
        grad = dot(lefts[n][part], right, TN)
        if received[n] is not None:
            grad += received[n][...].astype(F32)
        outs[n][...] = grad.astype(BF16)


def combine(experts, half, tp, core_ref, routes_ref, x_ref, out_ref):
    rows = routes_ref.shape[1]
    width = tp * LANES
    slots = slots_of(core_ref[0], routes_ref[...], experts, half)
    masks = masks_of(slots, experts * half)
    pick = functools.reduce(lambda a, m: jnp.where(m, 1.0, a), masks, jnp.zeros(masks[0].shape, F32))
    grads = dot(pick.astype(BF16), x_ref[:, :width], TN).astype(BF16)
    gate = x_ref[:, width : width + 1].astype(F32)
    lines = []
    for mask in masks:
        line = jnp.sum(jnp.where(mask, gate, 0.0), axis=0, keepdims=True)
        line = jnp.concatenate([line, jnp.zeros((1, 2 * LANES - rows), F32)], axis=1)
        lines += [line[:, :LANES], line[:, LANES:]]
    lines.append(jnp.zeros((16 - len(lines), LANES), F32))
    tail = jnp.concatenate(lines, axis=0).astype(BF16)
    for t in range(tp):
        out_ref[t, :rows, :] = grads[:, t * LANES : (t + 1) * LANES]
        out_ref[t, rows:, :] = tail


def finish(gates_ref, x_ref, tok_ref, gate_ref):
    top_k, rows = gates_ref.shape
    total = jnp.sum(x_ref[...].astype(F32), axis=0)
    tok_ref[...] = total[:rows].astype(BF16)
    gates = gates_ref[...].astype(F32)
    for k in range(top_k):
        line = jnp.concatenate(
            [total[rows + 2 * k : rows + 2 * k + 1], total[rows + 2 * k + 1 : rows + 2 * k + 2]],
            axis=1,
        )
        gate_ref[k : k + 1, :] = line[:, :rows] / gates[k : k + 1, :]


def local(experts, tp, tokens, cotangent, routing, gate_weights, gate_proj, up_proj, down_proj):
    rows, width = tokens.shape
    top_k = routing.shape[1]
    half = rows * top_k // experts
    count = experts * half
    core = lax.axis_index("c").astype(jnp.int32).reshape(1)
    routes, gates = routing.T, gate_weights.T
    swap = lambda v: lax.ppermute(v, "c", [(0, 1), (1, 0)])

    own = (gate_proj[0].T, up_proj[0].T, down_proj[0])
    other = tuple(swap(w) for w in own)
    ff = own[0].shape[0]

    sent = call(
        functools.partial(prepare, experts, half),
        jax.ShapeDtypeStruct((count, 2 * width), BF16),
        core, routes, gates, tokens, cotangent,
        in_specs=[SMEM, VMEM, VMEM, VMEM, VMEM],
        flops=4 * count * rows * width,
    )
    got = lax.all_to_all(
        sent.reshape(experts, half, 2 * width), EP, split_axis=0, concat_axis=0, tiled=True
    ).reshape(count, 2 * width)

    mid = jax.ShapeDtypeStruct((2, count, ff), BF16)
    back, hid, pre, up = call(
        expert,
        (jax.ShapeDtypeStruct((count, width + LANES), BF16), mid, mid, mid),
        got, *own, *other,
        flops=20 * count * width * ff,
    )
    returned = lax.all_to_all(
        back.reshape(experts, half, width + LANES), EP, split_axis=0, concat_axis=0, tiled=True
    ).reshape(count, width + LANES)

    shard = (jax.ShapeDtypeStruct((ff, width), BF16),) * 3
    theirs = call(
        functools.partial(weight_grads, 1, width), shard, got, hid, pre, up,
        flops=6 * count * width * ff,
    )
    received = tuple(swap(g) for g in theirs)
    grad_gate, grad_up, grad_down = call(
        functools.partial(weight_grads, 0, width), shard, got, hid, pre, up, *received,
        flops=6 * count * width * ff,
    )

    pieces = call(
        functools.partial(combine, experts, half, tp),
        jax.ShapeDtypeStruct((tp, rows + 16, LANES), BF16),
        core, routes, returned,
        in_specs=[SMEM, VMEM, VMEM],
        flops=2 * count * rows * width,
    )
    summed = lax.all_to_all(pieces, ("z", "c"), split_axis=0, concat_axis=0, tiled=True)
    grad_tokens, grad_gates = call(
        finish,
        (jax.ShapeDtypeStruct((rows, LANES), BF16), jax.ShapeDtypeStruct((top_k, rows), F32)),
        gates, summed,
    )
    return (grad_tokens, grad_gates.T, grad_gate.T[None], grad_up.T[None], grad_down[None])


def solution(mesh):
    devices = mesh.devices.reshape(4, 4, 8, 2)
    inner = jax.sharding.Mesh(devices, ("y", "x", "z", "c"))
    ep, tp = EP, ("z", "c")
    return jax.shard_map(
        functools.partial(local, 16, 16),
        mesh=inner,
        in_specs=(
            P(ep, None),
            P(ep, None),
            P(ep, None),
            P(ep, None),
            P(ep, None, tp),
            P(ep, None, tp),
            P(ep, tp, None),
        ),
        out_specs=(
            P(ep, tp),
            P(ep, None),
            P(ep, None, tp),
            P(ep, None, tp),
            P(ep, tp, None),
        ),
        check_vma=False,
    )
```

```python
import functools

import jax
import jax.numpy as jnp
from jax import lax
from jax.experimental import pallas as pl
from jax.experimental.pallas import tpu as pltpu
from jax.sharding import PartitionSpec as P

EP = ("y", "x")
LANES = 128
BF16 = jnp.bfloat16
F32 = jnp.float32
NN = (((1,), (0,)), ((), ()))
NT = (((1,), (1,)), ((), ()))
TN = (((0,), (0,)), ((), ()))
IN_VMEM = pl.BlockSpec(memory_space=pltpu.VMEM)
IN_HBM = pl.BlockSpec(memory_space=pltpu.HBM)
IN_SMEM = pl.BlockSpec(memory_space=pltpu.SMEM)


def dot(a, b, dims):
    return lax.dot_general(a, b, dims, preferred_element_type=F32)


def call(kernel, outs, *args, scratch=(), flops=0, mib=24):
    place = {"v": pltpu.VMEM, "h": pltpu.HBM, "w": pltpu.HBM}
    spec = {"v": IN_VMEM, "w": IN_VMEM, "h": IN_HBM, "s": IN_SMEM}
    moved = sum(a.size * a.dtype.itemsize for a, _ in args)
    return pl.pallas_call(
        kernel,
        out_shape=[place[m](shape, dtype) for shape, dtype, m in outs],
        in_specs=[spec[m] for _, m in args],
        out_specs=[spec[m] for _, _, m in outs],
        scratch_shapes=list(scratch),
        cost_estimate=pl.CostEstimate(flops=flops, bytes_accessed=moved, transcendentals=0),
        compiler_params=pltpu.CompilerParams(vmem_limit_bytes=mib * 1024 * 1024),
    )(*(a if m == "s" else pltpu.with_memory_space_constraint(a, place[m]) for a, m in args))


def slots_of(core, routes, experts, half):
    top_k, rows = routes.shape
    expert = lax.broadcasted_iota(jnp.int32, (experts, rows), 0)
    hits = [routes[k : k + 1, :] == expert for k in range(top_k)]
    named = functools.reduce(jnp.logical_or, hits)
    before = lax.broadcasted_iota(jnp.int32, (rows, rows), 0) < lax.broadcasted_iota(
        jnp.int32, (rows, rows), 1
    )
    ones = lambda mask: jnp.where(mask, 1.0, 0.0).astype(BF16)
    count = dot(ones(named), ones(before), NN)
    slots = []
    for k in range(top_k):
        place = jnp.sum(jnp.where(hits[k], count, 0.0), axis=0, keepdims=True).astype(jnp.int32)
        place = place - core * half
        inside = (place >= 0) & (place < half)
        slots.append(jnp.where(inside, routes[k : k + 1, :] * half + place, -1))
    return slots


def masks_of(slots, count):
    row = lax.broadcasted_iota(jnp.int32, (count, slots[0].shape[1]), 0)
    return [row == s for s in slots]


def send_tokens(experts, half, core_ref, par_ref, routes_ref, tok_ref, out_ref, tok, sem):
    part = out_ref.shape[1]
    copy = pltpu.make_async_copy(
        tok_ref.at[:, pl.ds(pl.multiple_of(par_ref[0] * part, part), part)], tok, sem
    )
    copy.start()
    masks = masks_of(slots_of(core_ref[0], routes_ref[...], experts, half), experts * half)
    pick = functools.reduce(lambda a, m: jnp.where(m, 1.0, a), masks, jnp.zeros(masks[0].shape, F32))
    copy.wait()
    out_ref[...] = dot(pick.astype(BF16), tok[...], NN).astype(BF16)


def send_cotangents(experts, half, core_ref, routes_ref, gates_ref, cot_ref, out_ref):
    masks = masks_of(slots_of(core_ref[0], routes_ref[...], experts, half), experts * half)
    gates = gates_ref[...].astype(F32)
    weigh = jnp.zeros(masks[0].shape, F32)
    for k, mask in enumerate(masks):
        weigh = jnp.where(mask, gates[k : k + 1, :], weigh)
    out_ref[...] = dot(weigh.astype(BF16), cot_ref[...], NN).astype(BF16)


def fetch(refs, buf, sem):
    copies = [pltpu.make_async_copy(r, buf.at[n], sem.at[n]) for n, r in enumerate(refs)]
    for copy in copies:
        copy.start()
    return copies


def forward(par_ref, mine_ref, low_ref, high_ref, *refs):
    weights, (hid_ref, slope_ref, act_ref, buf, sem) = refs[:4], refs[4:]
    copies = fetch(weights, buf, sem)
    rows, part = low_ref.shape
    here = pl.ds(pl.multiple_of(par_ref[0] * part, part), part)
    there = pl.ds(pl.multiple_of((1 - par_ref[0]) * part, part), part)

    def product(n):
        copies[n].wait()
        own = dot(mine_ref[...], buf[n, :, here], NT)
        other = buf[n, :, there]
        return own + jnp.concatenate(
            [dot(low_ref[...], other, NT), dot(high_ref[...], other, NT)], axis=0
        )

    for p in range(2):
        pre = product(2 * p)
        up = product(2 * p + 1)
        sig = jax.nn.sigmoid(pre)
        act = pre * sig
        hid_ref[p] = (act * up).astype(BF16)
        slope_ref[p] = up * sig * (1.0 + pre * (1.0 - sig))
        act_ref[p] = act


def backward(cot_ref, hid_ref, slope_ref, act_ref, *refs):
    weights, (back_ref, pre_ref, up_ref, *scratch) = refs[:6], refs[6:]
    buf, sem, hid, slope, act, mid_sem, pre, up, stage, out_sem = scratch
    copies = fetch(weights[:2], buf.at[:2], sem)
    mids = [
        pltpu.make_async_copy(ref, to, mid_sem.at[n])
        for n, (ref, to) in enumerate(((hid_ref, hid), (slope_ref, slope), (act_ref, act)))
    ]
    for mid in mids:
        mid.start()
    copies += fetch(weights[2:], buf.at[2:], sem.at[2:])
    rows, width = cot_ref.shape
    gate = jnp.zeros((rows, 1), F32)
    outs = []
    for p in range(2):
        copies[p].wait()
        back = dot(cot_ref[...], buf[p], NT)
        if p == 0:
            for mid in mids:
                mid.wait()
        gate = gate + jnp.sum(hid[p].astype(F32) * back, axis=1, keepdims=True)
        pre[p] = (back * slope[p]).astype(BF16)
        up[p] = (back * act[p]).astype(BF16)
        for n, (frm, to) in enumerate(((pre, pre_ref), (up, up_ref))):
            outs.append(pltpu.make_async_copy(frm.at[p], to.at[p], out_sem.at[2 * p + n]))
            outs[-1].start()
    for copy in copies[2:]:
        copy.wait()
    stage[:, width:] = jnp.broadcast_to(gate, (rows, LANES)).astype(BF16)
    step = width // 4
    for n in range(4):
        cols = slice(n * step, (n + 1) * step)
        total = dot(pre[0], buf[2, :, cols], NN)
        total += dot(up[0], buf[3, :, cols], NN)
        total += dot(pre[1], buf[4, :, cols], NN)
        total += dot(up[1], buf[5, :, cols], NN)
        stage[:, cols] = total.astype(BF16)
        span = slice(n * step, (n + 1) * step if n < 3 else width + LANES)
        outs.append(pltpu.make_async_copy(stage.at[:, span], back_ref.at[:, span], out_sem.at[4 + n]))
        outs[-1].start()
    for out in outs:
        out.wait()


def weight_grads(p, par_ref, mine_ref, low_ref, high_ref, cot_ref, hid_ref, pre_ref, up_ref, *refs):
    received, outs = (refs[:3], refs[3:]) if len(refs) > 3 else ((None,) * 3, refs)
    rows, part = low_ref.shape
    here = pl.ds(pl.multiple_of(par_ref[0] * part, part), part)
    there = pl.ds(pl.multiple_of((1 - par_ref[0]) * part, part), part)

    def put(n, cols, grad):
        if received[n] is not None:
            grad += received[n][:, cols].astype(F32)
        outs[n][:, cols] = grad.astype(BF16)

    for n, left in enumerate((pre_ref, up_ref)):
        put(n, here, dot(left[p], mine_ref[...], TN))
        grad = dot(left[p, :rows], low_ref[...], TN) + dot(left[p, rows:], high_ref[...], TN)
        put(n, there, grad)
    put(2, slice(None), dot(hid_ref[p], cot_ref[...], TN))


def combine(experts, half, core_ref, routes_ref, x_ref, keep_ref, send_ref):
    blocks, padded, _ = keep_ref.shape
    rows = routes_ref.shape[1]
    width = 2 * blocks * LANES
    core = core_ref[0]
    masks = masks_of(slots_of(core, routes_ref[...], experts, half), experts * half)
    pick = functools.reduce(lambda a, m: jnp.where(m, 1.0, a), masks, jnp.zeros(masks[0].shape, F32))
    grads = dot(pick.astype(BF16), x_ref[:, :width], TN)
    gate = x_ref[:, width : width + 1].astype(F32)
    lines = []
    for mask in masks:
        line = jnp.sum(jnp.where(mask, gate, 0.0), axis=0, keepdims=True)
        line = jnp.concatenate([line, jnp.zeros((1, 2 * LANES - rows), F32)], axis=1)
        lines += [line[:, :LANES], line[:, LANES:]]
    lines.append(jnp.zeros((padded - rows - len(lines), LANES), F32))
    tail = jnp.concatenate(lines, axis=0)
    for b in range(blocks):
        first = grads[:, 2 * b * LANES : (2 * b + 1) * LANES]
        second = grads[:, (2 * b + 1) * LANES : (2 * b + 2) * LANES]
        keep_ref[b, :rows, :] = jnp.where(core == 0, first, second)
        send_ref[b, :rows, :] = jnp.where(core == 0, second, first).astype(BF16)
        keep_ref[b, rows:, :] = tail
        send_ref[b, rows:, :] = tail.astype(BF16)


def join(keep_ref, got_ref, out_ref):
    out_ref[...] = (keep_ref[...] + got_ref[...].astype(F32)).astype(BF16)


def finish(gates_ref, x_ref, tok_ref, gate_ref):
    top_k, rows = gates_ref.shape
    total = jnp.sum(x_ref[...].astype(F32), axis=0)
    tok_ref[...] = total[:rows].astype(BF16)
    gates = gates_ref[...].astype(F32)
    for k in range(top_k):
        line = jnp.concatenate(
            [total[rows + 2 * k : rows + 2 * k + 1], total[rows + 2 * k + 1 : rows + 2 * k + 2]],
            axis=1,
        )
        gate_ref[k : k + 1, :] = line[:, :rows] / gates[k : k + 1, :]


def local(experts, tokens, cotangent, routing, gate_weights, gate_proj, up_proj, down_proj):
    rows, width = tokens.shape
    top_k = routing.shape[1]
    half = rows * top_k // experts
    count = experts * half
    part = width // 2
    depth = lax.axis_size("z")
    core = lax.axis_index("c").astype(jnp.int32).reshape(1)
    parity = (lax.axis_index("z") % 2).astype(jnp.int32).reshape(1)
    routes, gates = routing.T, gate_weights.T
    swap = lambda v: lax.ppermute(v, "c", [(0, 1), (1, 0)])
    shift = lambda v, k: lax.ppermute(v, "z", [(i, (i + k) % depth) for i in range(depth)])
    exchange = lambda v, axis: lax.all_to_all(v, axis, split_axis=0, concat_axis=0, tiled=True)
    dma = lambda n: pltpu.SemaphoreType.DMA((n,))

    own = (gate_proj[0].T, up_proj[0].T, down_proj[0])
    other = tuple(swap(w) for w in own)
    ff = own[0].shape[0]

    (tok_out,) = call(
        functools.partial(send_tokens, experts, half),
        [((count, part), BF16, "w")],
        (core, "s"), (parity, "s"), (routes, "w"), (tokens, "h"),
        scratch=[pltpu.VMEM((rows, part), BF16), pltpu.SemaphoreType.DMA],
        flops=2 * count * rows * part, mib=8,
    )
    mine = exchange(tok_out.reshape(experts, half, part), EP).reshape(count, part)
    (cot_out,) = call(
        functools.partial(send_cotangents, experts, half),
        [((count, width), BF16, "w")],
        (core, "s"), (routes, "w"), (gates, "w"), (cotangent, "w"),
        flops=2 * count * rows * width, mib=8,
    )
    cot = exchange(cot_out.reshape(experts, half, width), EP).reshape(count, width)
    low = shift(mine[: count // 2], 1)
    high = shift(mine[count // 2 :], -1)

    mid = lambda dtype, mode: ((2, count, ff), dtype, mode)
    hid, slope, act = call(
        forward,
        [mid(BF16, "w"), mid(F32, "w"), mid(F32, "w")],
        (parity, "s"), (mine, "v"), (low, "v"), (high, "v"),
        (own[0], "h"), (own[1], "h"), (other[0], "h"), (other[1], "h"),
        scratch=[pltpu.VMEM((4, ff, width), BF16), dma(4)],
        flops=8 * count * width * ff, mib=20,
    )
    mids = [pltpu.VMEM((2, count, ff), dtype) for dtype in (BF16, F32, F32)]
    back, pre, up = call(
        backward,
        [((count, width + LANES), BF16, "h"), mid(BF16, "h"), mid(BF16, "h")],
        (cot, "v"), (hid, "h"), (slope, "h"), (act, "h"),
        *((w, "h") for w in (own[2], other[2], own[0], own[1], other[0], other[1])),
        scratch=[
            pltpu.VMEM((6, ff, width), BF16), dma(6), *mids, dma(3),
            mids[0], mids[0], pltpu.VMEM((count, width + LANES), BF16), dma(8),
        ],
        flops=12 * count * width * ff, mib=28,
    )
    returned = exchange(back.reshape(experts, half, width + LANES), EP).reshape(count, width + LANES)

    pieces = [(v, "v") for v in (mine, low, high, cot)] + [(v, "w") for v in (hid, pre, up)]
    shard = [((ff, width), BF16, "w")] * 3
    theirs = call(
        functools.partial(weight_grads, 1), shard, (parity, "s"), *pieces,
        flops=6 * count * width * ff, mib=16,
    )
    received = [(swap(g), "w") for g in theirs]
    grad_gate, grad_up, grad_down = call(
        functools.partial(weight_grads, 0), shard, (parity, "s"), *pieces, *received,
        flops=6 * count * width * ff, mib=24,
    )

    block = (depth, rows + 16, LANES)
    keep, send = call(
        functools.partial(combine, experts, half),
        [(block, F32, "v"), (block, BF16, "v")],
        (core, "s"), (routes, "w"), (returned, "v"),
        flops=2 * count * rows * width, mib=12,
    )
    (joined,) = call(join, [(block, BF16, "w")], (keep, "v"), (swap(send), "v"), mib=4)
    summed = exchange(joined, "z")
    grad_tokens, grad_gates = call(
        finish,
        [((rows, LANES), BF16, "w"), ((top_k, rows), F32, "w")],
        (gates, "w"), (summed, "v"), mib=4,
    )
    return (grad_tokens, grad_gates.T, grad_gate.T[None], grad_up.T[None], grad_down[None])


def solution(mesh):
    devices = mesh.devices.reshape(4, 4, 8, 2)
    inner = jax.sharding.Mesh(devices, ("y", "x", "z", "c"))
    ep, tp = EP, ("z", "c")
    return jax.shard_map(
        functools.partial(local, 16),
        mesh=inner,
        in_specs=(
            P(ep, None),
            P(ep, None),
            P(ep, None),
            P(ep, None),
            P(ep, None, tp),
            P(ep, None, tp),
            P(ep, tp, None),
        ),
        out_specs=(
            P(ep, tp),
            P(ep, None),
            P(ep, None, tp),
            P(ep, None, tp),
            P(ep, tp, None),
        ),
        check_vma=False,
    )
```

```python
import functools

import jax
import jax.numpy as jnp
from jax import lax
from jax.experimental import pallas as pl
from jax.experimental.pallas import tpu as pltpu
from jax.sharding import PartitionSpec as P


EP = ("y", "x")
LANES = 128
BF16 = jnp.bfloat16
F32 = jnp.float32
NN = (((1,), (0,)), ((), ()))
NT = (((1,), (1,)), ((), ()))
TN = (((0,), (0,)), ((), ()))
IN_VMEM = pl.BlockSpec(memory_space=pltpu.VMEM)
IN_HBM = pl.BlockSpec(memory_space=pltpu.HBM)
IN_SMEM = pl.BlockSpec(memory_space=pltpu.SMEM)


def dot(a, b, dims):
    return lax.dot_general(a, b, dims, preferred_element_type=F32)


def call(kernel, outs, *args, scratch=(), flops=0, mib=24):
    place = {"v": pltpu.VMEM, "h": pltpu.HBM, "w": pltpu.HBM}
    spec = {"v": IN_VMEM, "w": IN_VMEM, "h": IN_HBM, "s": IN_SMEM}
    moved = sum(a.size * a.dtype.itemsize for a, _ in args)
    kernel_call = pl.pallas_call(
        kernel,
        out_shape=[place[m](shape, dtype) for shape, dtype, m in outs],
        in_specs=[spec[m] for _, m in args],
        out_specs=[spec[m] for _, _, m in outs],
        scratch_shapes=list(scratch),
        cost_estimate=pl.CostEstimate(flops=flops, bytes_accessed=moved, transcendentals=0),
        compiler_params=pltpu.CompilerParams(vmem_limit_bytes=mib * 1024 * 1024),
    )
    return kernel_call(
        *(a if m == "s" else pltpu.with_memory_space_constraint(a, place[m]) for a, m in args)
    )


def slots_of(core, routes, experts, half):
    top_k, rows = routes.shape
    expert = lax.broadcasted_iota(jnp.int32, (experts, rows), 0)
    hits = [routes[k : k + 1, :] == expert for k in range(top_k)]
    named = functools.reduce(jnp.logical_or, hits)
    before = lax.broadcasted_iota(jnp.int32, (rows, rows), 0) < lax.broadcasted_iota(
        jnp.int32, (rows, rows), 1
    )
    ones = lambda mask: jnp.where(mask, 1.0, 0.0).astype(BF16)
    count = dot(ones(named), ones(before), NN)
    slots = []
    for k in range(top_k):
        place = jnp.sum(jnp.where(hits[k], count, 0.0), axis=0, keepdims=True).astype(jnp.int32)
        place = place - core * half
        inside = (place >= 0) & (place < half)
        slots.append(jnp.where(inside, routes[k : k + 1, :] * half + place, -1))
    return slots


def masks_of(slots, count):
    row = lax.broadcasted_iota(jnp.int32, (count, slots[0].shape[1]), 0)
    return [row == s for s in slots]


def send_tokens(experts, half, core_ref, par_ref, routes_ref, tok_ref, out_ref, tok, sem):
    part = out_ref.shape[1]
    copy = pltpu.make_async_copy(
        tok_ref.at[:, pl.ds(pl.multiple_of(par_ref[0] * part, part), part)], tok, sem
    )
    copy.start()
    masks = masks_of(slots_of(core_ref[0], routes_ref[...], experts, half), experts * half)
    pick = functools.reduce(lambda a, m: jnp.where(m, 1.0, a), masks, jnp.zeros(masks[0].shape, F32))
    copy.wait()
    out_ref[...] = dot(pick.astype(BF16), tok[...], NN).astype(BF16)


def send_cotangents(experts, half, core_ref, routes_ref, gates_ref, cot_ref, out_ref):
    masks = masks_of(slots_of(core_ref[0], routes_ref[...], experts, half), experts * half)
    gates = gates_ref[...].astype(F32)
    weigh = jnp.zeros(masks[0].shape, F32)
    for k, mask in enumerate(masks):
        weigh = jnp.where(mask, gates[k : k + 1, :], weigh)
    out_ref[...] = dot(weigh.astype(BF16), cot_ref[...], NN).astype(BF16)


def join_rows(low_ref, high_ref, both):
    rows = low_ref.shape[0]
    both[:rows] = low_ref[...]
    both[rows:] = high_ref[...]


def forward(par_ref, mine_ref, low_ref, high_ref, *refs):
    weights, outs, (buf, sem, both, *stages, out_sem) = refs[:4], refs[4:7], refs[7:]
    copies = [pltpu.make_async_copy(w, buf.at[n], sem.at[n]) for n, w in enumerate(weights)]
    copies[0].start()
    copies[1].start()
    join_rows(low_ref, high_ref, both)
    part = low_ref.shape[1]
    here = pl.ds(pl.multiple_of(par_ref[0] * part, part), part)
    there = pl.ds(pl.multiple_of((1 - par_ref[0]) * part, part), part)

    def product(n):
        copies[n].wait()
        if n + 2 < 4:
            copies[n + 2].start()
        return dot(mine_ref[...], buf[n, :, here], NT) + dot(both[...], buf[n, :, there], NT)

    done = []
    for p in range(2):
        pre = product(2 * p)
        up = product(2 * p + 1)
        sig = jax.nn.sigmoid(pre)
        act = pre * sig
        stages[0][p] = (act * up).astype(BF16)
        stages[1][p] = up * sig * (1.0 + pre * (1.0 - sig))
        stages[2][p] = act
        for n in range(3):
            copy = pltpu.make_async_copy(stages[n].at[p], outs[n].at[p], out_sem.at[3 * p + n])
            copy.start()
            done.append(copy)
    for copy in done:
        copy.wait()


def gather_columns(weights, buf, sem, side, width):
    step = width // 8
    copies = []
    for n, w in enumerate(weights):
        for m in range(4):
            cols = pl.ds(pl.multiple_of((2 * m + side) * step, step), step)
            to = buf.at[n, :, m * step : (m + 1) * step]
            copies.append(pltpu.make_async_copy(w.at[:, cols], to, sem.at[4 * n + m]))
    return copies


def input_grad(pre, up, buf):
    total = dot(pre[0], buf[0], NN)
    total += dot(up[0], buf[1], NN)
    total += dot(pre[1], buf[2], NN)
    return total + dot(up[1], buf[3], NN)


def backward(par_ref, cot_ref, *refs):
    mid_refs, down, weights, outs, scratch = refs[:3], refs[3:5], refs[5:9], refs[9:14], refs[14:]
    low_ref, high_ref, pre_ref, up_ref, gate_ref = outs
    hid, slope, act, mid_sem, wd, wd_sem, buf, sem, pre, up, out_sem = scratch
    rows, width = cot_ref.shape
    mid_copies = [
        [pltpu.make_async_copy(r.at[p], to.at[p], mid_sem.at[3 * p + n])
         for n, (r, to) in enumerate(zip(mid_refs, (hid, slope, act)))]
        for p in range(2)
    ]
    downs = [pltpu.make_async_copy(w, wd.at[p], wd_sem.at[p]) for p, w in enumerate(down)]
    columns = gather_columns(weights, buf, sem, 1 - par_ref[0], width)
    downs[0].start()
    for copy in mid_copies[0]:
        copy.start()
    downs[1].start()
    gate = jnp.zeros((rows, 1), F32)
    done = []
    for p in range(2):
        downs[p].wait()
        for copy in mid_copies[1] if p == 0 else columns:
            copy.start()
        back = dot(cot_ref[...], wd[p], NT)
        for copy in mid_copies[p]:
            copy.wait()
        gate = gate + jnp.sum(hid[p].astype(F32) * back, axis=1, keepdims=True)
        pre[p] = (back * slope[p]).astype(BF16)
        up[p] = (back * act[p]).astype(BF16)
        for n, (frm, to) in enumerate(((pre, pre_ref), (up, up_ref))):
            copy = pltpu.make_async_copy(frm.at[p], to.at[p], out_sem.at[2 * p + n])
            copy.start()
            done.append(copy)
    for copy in columns:
        copy.wait()
    total = input_grad(pre, up, buf).astype(BF16)
    wide = jnp.broadcast_to(gate, (rows, LANES))
    gate_ref[...] = wide
    low_ref[:, : width // 2] = total[: rows // 2]
    low_ref[:, width // 2 :] = wide[: rows // 2].astype(BF16)
    high_ref[:, : width // 2] = total[rows // 2 :]
    high_ref[:, width // 2 :] = wide[rows // 2 :].astype(BF16)
    for copy in done:
        copy.wait()


def own_half(par_ref, pre_ref, up_ref, gate_ref, *refs):
    weights, (out_ref, buf, sem) = refs[:4], refs[4:]
    half = buf.shape[2]
    columns = gather_columns(weights, buf, sem, par_ref[0], 2 * half)
    for copy in columns:
        copy.start()
    for copy in columns:
        copy.wait()
    out_ref[:, :half] = input_grad(pre_ref, up_ref, buf)
    out_ref[:, half:] = gate_ref[...]


def add_pair(own_ref, low_ref, high_ref, out_ref):
    rows = low_ref.shape[0]
    out_ref[:rows] = (own_ref[:rows] + low_ref[...].astype(F32)).astype(BF16)
    out_ref[rows:] = (own_ref[rows:] + high_ref[...].astype(F32)).astype(BF16)


def weight_grads(p, par_ref, mine_ref, low_ref, high_ref, cot_ref, hid_ref, pre_ref, up_ref, *refs):
    both = refs[-1]
    received, outs = (refs[:3], refs[3:6]) if len(refs) > 4 else ((None,) * 3, refs[:3])
    join_rows(low_ref, high_ref, both)
    part = low_ref.shape[1]
    here = pl.ds(pl.multiple_of(par_ref[0] * part, part), part)
    there = pl.ds(pl.multiple_of((1 - par_ref[0]) * part, part), part)

    def put(n, cols, grad):
        if received[n] is not None:
            grad += received[n][:, cols].astype(F32)
        outs[n][:, cols] = grad.astype(BF16)

    for n, left in enumerate((pre_ref, up_ref)):
        put(n, here, dot(left[p], mine_ref[...], TN))
        put(n, there, dot(left[p], both[...], TN))
    put(2, slice(None), dot(hid_ref[p], cot_ref[...], TN))


def combine(experts, half, core_ref, routes_ref, x_ref, keep_ref, send_ref):
    blocks, padded, _ = keep_ref.shape
    rows = routes_ref.shape[1]
    width = 2 * blocks * LANES
    core = core_ref[0]
    masks = masks_of(slots_of(core, routes_ref[...], experts, half), experts * half)
    pick = functools.reduce(lambda a, m: jnp.where(m, 1.0, a), masks, jnp.zeros(masks[0].shape, F32))
    grads = dot(pick.astype(BF16), x_ref[:, :width], TN)
    gate = x_ref[:, width : width + 1].astype(F32)
    lines = []
    for mask in masks:
        line = jnp.sum(jnp.where(mask, gate, 0.0), axis=0, keepdims=True)
        line = jnp.concatenate([line, jnp.zeros((1, 2 * LANES - rows), F32)], axis=1)
        lines += [line[:, :LANES], line[:, LANES:]]
    lines.append(jnp.zeros((padded - rows - len(lines), LANES), F32))
    tail = jnp.concatenate(lines, axis=0)
    for b in range(blocks):
        first = grads[:, 2 * b * LANES : (2 * b + 1) * LANES]
        second = grads[:, (2 * b + 1) * LANES : (2 * b + 2) * LANES]
        keep_ref[b, :rows, :] = jnp.where(core == 0, first, second)
        send_ref[b, :rows, :] = jnp.where(core == 0, second, first).astype(BF16)
        keep_ref[b, rows:, :] = tail
        send_ref[b, rows:, :] = tail.astype(BF16)


def join(turn_ref, keep_ref, got_ref, *out_refs):
    for k, out_ref in enumerate(out_refs):
        block = lax.rem(turn_ref[0] + k, len(out_refs))
        out_ref[...] = (keep_ref[block] + got_ref[block].astype(F32)).astype(BF16)


def finish(gates_ref, *refs):
    parts, (tok_ref, gate_ref) = refs[:-2], refs[-2:]
    top_k, rows = gates_ref.shape
    total = functools.reduce(jnp.add, [x[...].astype(F32) for x in parts])
    tok_ref[...] = total[:rows].astype(BF16)
    gates = gates_ref[...].astype(F32)
    for k in range(top_k):
        line = jnp.concatenate(
            [total[rows + 2 * k : rows + 2 * k + 1], total[rows + 2 * k + 1 : rows + 2 * k + 2]],
            axis=1,
        )
        gate_ref[k : k + 1, :] = line[:, :rows] / gates[k : k + 1, :]


def local(experts, tokens, cotangent, routing, gate_weights, gate_proj, up_proj, down_proj):
    rows, width = tokens.shape
    top_k = routing.shape[1]
    half = rows * top_k // experts
    count = experts * half
    part = width // 2
    depth = lax.axis_size("z")
    core = lax.axis_index("c").astype(jnp.int32).reshape(1)
    parity = (lax.axis_index("z") % 2).astype(jnp.int32).reshape(1)
    routes, gates = routing.T, gate_weights.T

    def swap(v):
        return lax.ppermute(v, "c", [(0, 1), (1, 0)])

    def shift(v, k):
        return lax.ppermute(v, "z", [(i, (i + k) % depth) for i in range(depth)])

    def exchange(v):
        return lax.all_to_all(v, EP, split_axis=0, concat_axis=0, tiled=True)

    dma = lambda n: pltpu.SemaphoreType.DMA((n,))

    own = (gate_proj[0].T, up_proj[0].T, down_proj[0])
    other = tuple(swap(w) for w in own)
    ff = own[0].shape[0]

    (tok_out,) = call(
        functools.partial(send_tokens, experts, half),
        [((count, part), BF16, "w")],
        (core, "s"), (parity, "s"), (routes, "w"), (tokens, "h"),
        scratch=[pltpu.VMEM((rows, part), BF16), pltpu.SemaphoreType.DMA],
        flops=2 * count * rows * part, mib=8,
    )
    mine = exchange(tok_out.reshape(experts, half, part)).reshape(count, part)
    (cot_out,) = call(
        functools.partial(send_cotangents, experts, half),
        [((count, width), BF16, "w")],
        (core, "s"), (routes, "w"), (gates, "w"), (cotangent, "w"),
        flops=2 * count * rows * width, mib=8,
    )
    cot = exchange(cot_out.reshape(experts, half, width)).reshape(count, width)
    low = shift(mine[: count // 2], 1)
    high = shift(mine[count // 2 :], -1)

    mid = lambda dtype, mode: ((2, count, ff), dtype, mode)
    mids = [pltpu.VMEM((2, count, ff), dtype) for dtype in (BF16, F32, F32)]
    proj = [(w, "h") for w in (own[0], own[1], other[0], other[1])]
    hid, slope, act = call(
        forward,
        [mid(BF16, "h"), mid(F32, "h"), mid(F32, "h")],
        (parity, "s"), (mine, "v"), (low, "v"), (high, "v"), *proj,
        scratch=[
            pltpu.VMEM((4, ff, width), BF16), dma(4), pltpu.VMEM((count, part), BF16),
            *mids, dma(6),
        ],
        flops=8 * count * width * ff, mib=24,
    )
    message = (count // 2, part + LANES)
    packed = [pltpu.VMEM((4, ff, part), BF16), dma(16)]
    to_low, to_high, pre, up, gate = call(
        backward,
        [(message, BF16, "v"), (message, BF16, "v"), mid(BF16, "h"), mid(BF16, "h"), ((count, LANES), F32, "w")],
        (parity, "s"), (cot, "v"), (hid, "h"), (slope, "h"), (act, "h"),
        (own[2], "h"), (other[2], "h"), *proj,
        scratch=[
            *mids, dma(6), pltpu.VMEM((2, ff, width), BF16), dma(2), *packed,
            mids[0], mids[0], dma(4),
        ],
        flops=8 * count * width * ff, mib=24,
    )
    from_low, from_high = shift(to_low, -1), shift(to_high, 1)
    (kept,) = call(
        own_half,
        [((count, part + LANES), F32, "v")],
        (parity, "s"), (pre, "w"), (up, "w"), (gate, "w"), *proj,
        scratch=packed,
        flops=4 * count * width * ff, mib=16,
    )
    (pair,) = call(
        add_pair, [((count, part + LANES), BF16, "w")], (kept, "v"), (from_low, "v"), (from_high, "v"), mib=8
    )
    returned = exchange(pair.reshape(experts, half, part + LANES)).reshape(count, part + LANES)

    pieces = [(v, "v") for v in (mine, low, high, cot)] + [(v, "w") for v in (hid, pre, up)]
    shard = [((ff, width), BF16, "w")] * 3
    theirs = call(
        functools.partial(weight_grads, 1), shard, (parity, "s"), *pieces,
        scratch=[pltpu.VMEM((count, part), BF16)],
        flops=6 * count * width * ff, mib=16,
    )
    received = [(swap(g), "w") for g in theirs]
    grad_gate, grad_up, grad_down = call(
        functools.partial(weight_grads, 0), shard, (parity, "s"), *pieces, *received,
        scratch=[pltpu.VMEM((count, part), BF16)],
        flops=6 * count * width * ff, mib=24,
    )

    steps = depth // 2
    block = (rows + 16, LANES)
    keep, send = call(
        functools.partial(combine, experts, half),
        [((steps, *block), F32, "v"), ((steps, *block), BF16, "v")],
        (core, "s"), (routes, "w"), (returned, "v"),
        flops=2 * count * rows * part, mib=12,
    )
    turn = (lax.axis_index("z") // 2).astype(jnp.int32).reshape(1)
    parts = call(join, [(block, BF16, "v")] * steps, (turn, "s"), (keep, "v"), (swap(send), "v"), mib=4)
    sums = [parts[0]] + [shift(parts[k], 2 * k) for k in range(1, steps)]
    grad_tokens, grad_gates = call(
        finish,
        [((rows, LANES), BF16, "w"), ((top_k, rows), F32, "w")],
        (gates, "w"), *((v, "v") for v in sums), mib=4,
    )
    return (grad_tokens, grad_gates.T, grad_gate.T[None], grad_up.T[None], grad_down[None])


def solution(mesh):
    devices = mesh.devices.reshape(4, 4, 8, 2)
    inner = jax.sharding.Mesh(devices, ("y", "x", "z", "c"))
    ep, tp = EP, ("z", "c")

    def body(*args):
        return local(16, *args)

    return jax.shard_map(
        body,
        mesh=inner,
        in_specs=(
            P(ep, None),
            P(ep, None),
            P(ep, None),
            P(ep, None),
            P(ep, None, tp),
            P(ep, None, tp),
            P(ep, tp, None),
        ),
        out_specs=(
            P(ep, tp),
            P(ep, None),
            P(ep, None, tp),
            P(ep, None, tp),
            P(ep, tp, None),
        ),
        check_vma=False,
    )
```

```python
import functools

import jax
import jax.numpy as jnp
from jax import lax
from jax.experimental import pallas as pl
from jax.experimental.pallas import tpu as pltpu
from jax.sharding import PartitionSpec as P


EP = ("y", "x")
Z = ("zh", "zl")
LANES = 128
BF16 = jnp.bfloat16
F32 = jnp.float32
NN = (((1,), (0,)), ((), ()))
NT = (((1,), (1,)), ((), ()))
TN = (((0,), (0,)), ((), ()))
IN_VMEM = pl.BlockSpec(memory_space=pltpu.VMEM)
IN_HBM = pl.BlockSpec(memory_space=pltpu.HBM)
IN_SMEM = pl.BlockSpec(memory_space=pltpu.SMEM)


def dot(a, b, dims):
    return lax.dot_general(a, b, dims, preferred_element_type=F32)


def call(kernel, outs, *args, scratch=(), flops=0, mib=24):
    place = {"v": pltpu.VMEM, "h": pltpu.HBM, "w": pltpu.HBM}
    spec = {"v": IN_VMEM, "w": IN_VMEM, "h": IN_HBM, "s": IN_SMEM}
    moved = sum(a.size * a.dtype.itemsize for a, _ in args)
    kernel_call = pl.pallas_call(
        kernel,
        out_shape=[place[m](shape, dtype) for shape, dtype, m in outs],
        in_specs=[spec[m] for _, m in args],
        out_specs=[spec[m] for _, _, m in outs],
        scratch_shapes=list(scratch),
        cost_estimate=pl.CostEstimate(flops=flops, bytes_accessed=moved, transcendentals=0),
        compiler_params=pltpu.CompilerParams(vmem_limit_bytes=mib * 1024 * 1024),
    )
    return kernel_call(
        *(a if m == "s" else pltpu.with_memory_space_constraint(a, place[m]) for a, m in args)
    )


def slots_of(core, routes, experts, half):
    top_k, rows = routes.shape
    expert = lax.broadcasted_iota(jnp.int32, (experts, rows), 0)
    hits = [routes[k : k + 1, :] == expert for k in range(top_k)]
    named = functools.reduce(jnp.logical_or, hits)
    before = lax.broadcasted_iota(jnp.int32, (rows, rows), 0) < lax.broadcasted_iota(
        jnp.int32, (rows, rows), 1
    )
    ones = lambda mask: jnp.where(mask, 1.0, 0.0).astype(BF16)
    count = dot(ones(named), ones(before), NN)
    slots = []
    for k in range(top_k):
        place = jnp.sum(jnp.where(hits[k], count, 0.0), axis=0, keepdims=True).astype(jnp.int32)
        place = place - core * half
        inside = (place >= 0) & (place < half)
        slots.append(jnp.where(inside, routes[k : k + 1, :] * half + place, -1))
    return slots


def masks_of(slots, count):
    row = lax.broadcasted_iota(jnp.int32, (count, slots[0].shape[1]), 0)
    return [row == s for s in slots]


def pick_of(masks):
    hit = functools.reduce(jnp.logical_or, masks)
    return jnp.where(hit, 1.0, 0.0).astype(BF16)


def send_tokens(experts, half, core_ref, par_ref, routes_ref, tok_ref, out_ref, tok, sem):
    copies = [
        pltpu.make_async_copy(tok_ref.at[:, cols], tok.at[:, to], sem.at[n])
        for n, (to, cols) in enumerate(side_columns(par_ref[0], tok_ref.shape[1]))
    ]
    for copy in copies:
        copy.start()
    masks = masks_of(slots_of(core_ref[0], routes_ref[...], experts, half), experts * half)
    for copy in copies:
        copy.wait()
    out_ref[...] = dot(pick_of(masks), tok[...], NN).astype(BF16)


def keep_table(experts, half, core_ref, routes_ref, gates_ref, out_ref):
    slots = slots_of(core_ref[0], routes_ref[...], experts, half)
    top_k = len(slots)
    gates = gates_ref[...].astype(F32)
    out_ref[...] = jnp.zeros(out_ref.shape, F32)
    for k in range(top_k):
        out_ref[k : k + 1] = slots[k].astype(F32)
        out_ref[top_k + k : top_k + k + 1] = gates[k : k + 1]


def table_slots(table_ref):
    return [table_ref[k : k + 1].astype(jnp.int32) for k in range(2)]


def send_cotangents(table_ref, cot_ref, out_ref):
    masks = masks_of(table_slots(table_ref), out_ref.shape[0])
    weigh = jnp.zeros(masks[0].shape, F32)
    for k, mask in enumerate(masks):
        weigh = jnp.where(mask, table_ref[2 + k : 3 + k], weigh)
    out_ref[...] = dot(weigh.astype(BF16), cot_ref[...], NN).astype(BF16)


def side_columns(side, width):
    step = width // 8
    return [
        (slice(m * step, (m + 1) * step), pl.ds(pl.multiple_of((2 * m + side) * step, step), step))
        for m in range(4)
    ]


def pack(par_ref, gate_ref, up_ref, out_ref, buf, sem, made, out_sem):
    copies = [pltpu.make_async_copy(w, buf.at[n], sem.at[n]) for n, w in enumerate((gate_ref, up_ref))]
    for copy in copies:
        copy.start()
    done = []
    for n, copy in enumerate(copies):
        copy.wait()
        for k in range(2):
            for to, cols in side_columns(jnp.where(k == 0, par_ref[0], 1 - par_ref[0]), buf.shape[2]):
                made[n, k, :, to] = buf[n, :, cols]
            done.append(pltpu.make_async_copy(made.at[n, k], out_ref.at[n, k], out_sem.at[2 * n + k]))
            done[-1].start()
    for copy in done:
        copy.wait()


def join_rows(low_ref, high_ref, both):
    rows = low_ref.shape[0]
    both[:rows] = low_ref[...]
    both[rows:] = high_ref[...]


def forward(mine_ref, low_ref, high_ref, own_ref, other_ref, out_ref, buf, sem, both, made, out_sem):
    jobs = [(w.at[n, k], buf.at[2 * p + n, k]) for p, w in enumerate((own_ref, other_ref)) for n in range(2) for k in range(2)]
    copies = [pltpu.make_async_copy(a, b, sem.at[i]) for i, (a, b) in enumerate(jobs)]
    for copy in copies[:4]:
        copy.start()
    join_rows(low_ref, high_ref, both)
    done = []

    def product(n):
        copies[2 * n].wait()
        copies[2 * n + 1].wait()
        for copy in copies[2 * n + 4 : 2 * n + 6]:
            copy.start()
        return dot(mine_ref[...], buf[n, 0], NT) + dot(both[...], buf[n, 1], NT)

    for p in range(2):
        pre = product(2 * p)
        up = product(2 * p + 1)
        sig = jax.nn.sigmoid(pre)
        act = pre * sig
        made[p, 0] = (act * up).astype(BF16)
        made[p, 1] = (up * sig * (1.0 + pre * (1.0 - sig))).astype(BF16)
        made[p, 2] = act.astype(BF16)
        done.append(pltpu.make_async_copy(made.at[p], out_ref.at[p], out_sem.at[p]))
        done[-1].start()
    for copy in done:
        copy.wait()


def input_grad(grads, buf):
    total = dot(grads[0, 0], buf[0], NN)
    total += dot(grads[0, 1], buf[1], NN)
    total += dot(grads[1, 0], buf[2], NN)
    return total + dot(grads[1, 1], buf[3], NN)


def fetch_half(k, own_ref, other_ref, buf, sem):
    return [
        pltpu.make_async_copy(w.at[n, k], buf.at[2 * p + n], sem.at[2 * p + n])
        for p, w in enumerate((own_ref, other_ref))
        for n in range(2)
    ]


def backward(cot_ref, mid_ref, down0_ref, down1_ref, own_ref, other_ref, low_ref, high_ref, grads_ref, gate_ref, mid, mid_sem, wd, wd_sem, buf, sem, grads, out_sem):
    rows, width = cot_ref.shape
    mids = [pltpu.make_async_copy(mid_ref.at[p], mid.at[p], mid_sem.at[p]) for p in range(2)]
    downs = [
        pltpu.make_async_copy(w, wd.at[p], wd_sem.at[p]) for p, w in enumerate((down0_ref, down1_ref))
    ]
    columns = fetch_half(1, own_ref, other_ref, buf, sem)
    downs[0].start()
    mids[0].start()
    downs[1].start()
    mids[1].start()
    gate = jnp.zeros((rows, 1), F32)
    done = []
    for p in range(2):
        downs[p].wait()
        for copy in columns[2 * p : 2 * p + 2]:
            copy.start()
        back = dot(cot_ref[...], wd[p], NT)
        mids[p].wait()
        gate = gate + jnp.sum(mid[p, 0].astype(F32) * back, axis=1, keepdims=True)
        grads[p, 0] = (back * mid[p, 1].astype(F32)).astype(BF16)
        grads[p, 1] = (back * mid[p, 2].astype(F32)).astype(BF16)
        done.append(pltpu.make_async_copy(grads.at[p], grads_ref.at[p], out_sem.at[p]))
        done[-1].start()
    wide = jnp.broadcast_to(gate, (rows, LANES))
    gate_ref[...] = wide
    low_ref[:, width // 2 :] = wide[: rows // 2].astype(BF16)
    high_ref[:, width // 2 :] = wide[rows // 2 :].astype(BF16)
    for copy in columns:
        copy.wait()
    total = input_grad(grads, buf).astype(BF16)
    low_ref[:, : width // 2] = total[: rows // 2]
    high_ref[:, : width // 2] = total[rows // 2 :]
    for copy in done:
        copy.wait()


def own_half(grads_ref, gate_ref, own_ref, other_ref, out_ref, grads, grad_sem, buf, sem):
    copies = [pltpu.make_async_copy(grads_ref.at[p], grads.at[p], grad_sem.at[p]) for p in range(2)]
    copies += fetch_half(0, own_ref, other_ref, buf, sem)
    for copy in copies:
        copy.start()
    part = buf.shape[2]
    out_ref[:, part:] = gate_ref[...]
    for copy in copies:
        copy.wait()
    out_ref[:, :part] = input_grad(grads, buf)


def add_pair(own_ref, low_ref, high_ref, out_ref):
    rows = low_ref.shape[0]
    out_ref[:rows] = (own_ref[:rows] + low_ref[...].astype(F32)).astype(BF16)
    out_ref[rows:] = (own_ref[rows:] + high_ref[...].astype(F32)).astype(BF16)


def weight_grads(p, par_ref, mine_ref, low_ref, high_ref, cot_ref, mid_ref, grads_ref, *refs):
    inputs = refs[:3] if p == 0 else ()
    outs, (both, made, out_sem, left, left_sem, *got) = refs[len(inputs) :][:3], refs[len(inputs) + 3 :]
    lefts = [grads_ref.at[p, 0], grads_ref.at[p, 1], mid_ref.at[p, 0]]
    copies = [pltpu.make_async_copy(r, left.at[n], left_sem.at[n]) for n, r in enumerate(lefts)]
    received = [pltpu.make_async_copy(r, got[0].at[n], got[1].at[n]) for n, r in enumerate(inputs)]
    for copy in copies + received:
        copy.start()
    join_rows(low_ref, high_ref, both)
    done = []

    def put(n, cols, grad):
        if p == 0:
            grad += got[0][n, :, cols].astype(F32)
        made[n, :, cols] = grad.astype(BF16)

    for n in range(3):
        copies[n].wait()
        if p == 0:
            received[n].wait()
        if n < 2:
            for side, right in ((par_ref[0], mine_ref), (1 - par_ref[0], both)):
                grad = dot(left[n], right[...], TN)
                for to, cols in side_columns(side, made.shape[2]):
                    put(n, cols, grad[:, to])
        else:
            put(n, slice(None), dot(left[n], cot_ref[...], TN))
        done.append(pltpu.make_async_copy(made.at[n], outs[n], out_sem.at[n]))
        done[-1].start()
    for copy in done:
        copy.wait()


def combine(core_ref, table_ref, x_ref, keep_ref, send_ref):
    blocks, padded, _ = keep_ref.shape
    rows = table_ref.shape[1]
    width = 2 * blocks * LANES
    core = core_ref[0]
    masks = masks_of(table_slots(table_ref), x_ref.shape[0])
    grads = dot(pick_of(masks), x_ref[:, :width], TN)
    gate = x_ref[:, width : width + 1].astype(F32)
    lines = []
    for mask in masks:
        line = jnp.sum(jnp.where(mask, gate, 0.0), axis=0, keepdims=True)
        line = jnp.concatenate([line, jnp.zeros((1, 2 * LANES - rows), F32)], axis=1)
        lines += [line[:, :LANES], line[:, LANES:]]
    lines.append(jnp.zeros((padded - rows - len(lines), LANES), F32))
    tail = jnp.concatenate(lines, axis=0)
    for b in range(blocks):
        first = grads[:, 2 * b * LANES : (2 * b + 1) * LANES]
        second = grads[:, (2 * b + 1) * LANES : (2 * b + 2) * LANES]
        keep_ref[b, :rows, :] = jnp.where(core == 0, first, second)
        send_ref[b, :rows, :] = jnp.where(core == 0, second, first).astype(BF16)
        keep_ref[b, rows:, :] = tail
        send_ref[b, rows:, :] = tail.astype(BF16)


def join(keep_ref, got_ref, out_ref):
    out_ref[...] = (keep_ref[...] + got_ref[...].astype(F32)).astype(BF16)


def finish(table_ref, x_ref, tok_ref, gate_ref):
    top_k, rows = gate_ref.shape
    total = jnp.sum(x_ref[...].astype(F32), axis=0)
    tok_ref[...] = total[:rows].astype(BF16)
    for k in range(top_k):
        line = jnp.concatenate(
            [total[rows + 2 * k : rows + 2 * k + 1], total[rows + 2 * k + 1 : rows + 2 * k + 2]],
            axis=1,
        )
        gate_ref[k : k + 1, :] = line[:, :rows] / table_ref[top_k + k : top_k + k + 1, :]


def local(experts, tokens, cotangent, routing, gate_weights, gate_proj, up_proj, down_proj):
    rows, width = tokens.shape
    top_k = routing.shape[1]
    half = rows * top_k // experts
    count = experts * half
    part = width // 2
    depth = lax.axis_size(Z)
    core = lax.axis_index("c").astype(jnp.int32).reshape(1)
    parity = (lax.axis_index(Z) % 2).astype(jnp.int32).reshape(1)
    routes, gates = routing.T, gate_weights.T

    def swap(v):
        return lax.ppermute(v, "c", [(0, 1), (1, 0)])

    def shift(v, k):
        return lax.ppermute(v, Z, [(i, (i + k) % depth) for i in range(depth)])

    def exchange(v):
        return lax.all_to_all(v, EP, split_axis=0, concat_axis=0, tiled=True)

    dma = lambda n: pltpu.SemaphoreType.DMA((n,))

    ff = gate_proj.shape[2]
    down = down_proj[0]
    down_other = swap(down)
    (own,) = call(
        pack, [((2, 2, ff, part), BF16, "h")],
        (parity, "s"), (gate_proj[0].T, "h"), (up_proj[0].T, "h"),
        scratch=[
            pltpu.VMEM((2, ff, width), BF16), dma(2), pltpu.VMEM((2, 2, ff, part), BF16), dma(4),
        ],
        mib=10,
    )
    other = swap(own)
    (table,) = call(
        functools.partial(keep_table, experts, half), [((8, rows), F32, "v")],
        (core, "s"), (routes, "w"), (gates, "w"), mib=4,
    )

    (tok_out,) = call(
        functools.partial(send_tokens, experts, half),
        [((count, part), BF16, "w")],
        (core, "s"), (parity, "s"), (routes, "w"), (tokens, "h"),
        scratch=[pltpu.VMEM((rows, part), BF16), dma(4)],
        flops=2 * count * rows * part, mib=8,
    )
    mine = exchange(tok_out.reshape(experts, half, part)).reshape(count, part)
    (cot_out,) = call(
        send_cotangents, [((count, width), BF16, "w")],
        (table, "v"), (cotangent, "w"),
        flops=2 * count * rows * width, mib=8,
    )
    cot = exchange(cot_out.reshape(experts, half, width)).reshape(count, width)
    low = shift(mine[: count // 2], 1)
    high = shift(mine[count // 2 :], -1)

    packed = [(own, "h"), (other, "h")]
    mids = pltpu.VMEM((2, 3, count, ff), BF16)
    halves = [pltpu.VMEM((4, ff, part), BF16), dma(4)]
    (mid,) = call(
        forward, [((2, 3, count, ff), BF16, "h")],
        (mine, "v"), (low, "v"), (high, "v"), *packed,
        scratch=[
            pltpu.VMEM((4, 2, ff, part), BF16), dma(8), pltpu.VMEM((count, part), BF16), mids, dma(2),
        ],
        flops=8 * count * width * ff, mib=18,
    )
    message = ((count // 2, part + LANES), BF16, "v")
    to_low, to_high, grads, gate = call(
        backward,
        [message, message, ((2, 2, count, ff), BF16, "h"), ((count, LANES), F32, "v")],
        (cot, "v"), (mid, "h"), (down, "h"), (down_other, "h"), *packed,
        scratch=[
            mids, dma(2), pltpu.VMEM((2, ff, width), BF16), dma(2), *halves,
            pltpu.VMEM((2, 2, count, ff), BF16), dma(2),
        ],
        flops=8 * count * width * ff, mib=20,
    )
    from_low, from_high = shift(to_low, -1), shift(to_high, 1)
    (kept,) = call(
        own_half, [((count, part + LANES), F32, "v")],
        (grads, "h"), (gate, "v"), *packed,
        scratch=[pltpu.VMEM((2, 2, count, ff), BF16), dma(2), *halves],
        flops=4 * count * width * ff, mib=14,
    )
    (pair,) = call(
        add_pair, [((count, part + LANES), BF16, "w")], (kept, "v"), (from_low, "v"), (from_high, "v"), mib=8
    )
    returned = exchange(pair.reshape(experts, half, part + LANES)).reshape(count, part + LANES)

    pieces = [(v, "v") for v in (mine, low, high, cot)] + [(v, "h") for v in (mid, grads)]
    shard = [((ff, width), BF16, "h")] * 3
    whole = pltpu.VMEM((3, ff, width), BF16)
    room = [pltpu.VMEM((count, part), BF16), whole, dma(3), pltpu.VMEM((3, count, ff), BF16), dma(3)]
    theirs = call(
        functools.partial(weight_grads, 1), shard, (parity, "s"), *pieces,
        scratch=room, flops=6 * count * width * ff, mib=14,
    )
    received = [(swap(g), "h") for g in theirs]
    grad_gate, grad_up, grad_down = call(
        functools.partial(weight_grads, 0), shard, (parity, "s"), *pieces, *received,
        scratch=[*room, whole, dma(3)], flops=6 * count * width * ff, mib=20,
    )

    block = (depth // 2, rows + 16, LANES)
    keep, send = call(
        combine, [(block, F32, "v"), (block, BF16, "v")],
        (core, "s"), (table, "v"), (returned, "v"),
        flops=2 * count * rows * part, mib=10,
    )
    (joined,) = call(join, [(block, BF16, "v")], (keep, "v"), (swap(send), "v"), mib=4)
    summed = lax.all_to_all(joined, "zh", split_axis=0, concat_axis=0, tiled=True)
    grad_tokens, grad_gates = call(
        finish,
        [((rows, LANES), BF16, "w"), ((top_k, rows), F32, "w")],
        (table, "v"), (summed, "v"), mib=4,
    )
    return (grad_tokens, grad_gates.T, grad_gate.T[None], grad_up.T[None], grad_down[None])


def solution(mesh):
    devices = mesh.devices.reshape(4, 4, 4, 2, 2)
    inner = jax.sharding.Mesh(devices, (*EP, *Z, "c"))
    ep, tp = EP, (*Z, "c")

    def body(*args):
        return local(16, *args)

    return jax.shard_map(
        body,
        mesh=inner,
        in_specs=(
            P(ep, None),
            P(ep, None),
            P(ep, None),
            P(ep, None),
            P(ep, None, tp),
            P(ep, None, tp),
            P(ep, tp, None),
        ),
        out_specs=(
            P(ep, tp),
            P(ep, None),
            P(ep, None, tp),
            P(ep, None, tp),
            P(ep, tp, None),
        ),
        check_vma=False,
    )
```

```python
import functools

import jax
import jax.numpy as jnp
from jax import lax
from jax.experimental import pallas as pl
from jax.experimental.pallas import tpu as pltpu
from jax.sharding import PartitionSpec as P


EP = ("y", "x")
Z = ("zh", "zl")
LANES = 128
BF16 = jnp.bfloat16
F32 = jnp.float32
NN = (((1,), (0,)), ((), ()))
NT = (((1,), (1,)), ((), ()))
TN = (((0,), (0,)), ((), ()))
IN_VMEM = pl.BlockSpec(memory_space=pltpu.VMEM)
IN_HBM = pl.BlockSpec(memory_space=pltpu.HBM)
IN_SMEM = pl.BlockSpec(memory_space=pltpu.SMEM)


def dot(a, b, dims):
    return lax.dot_general(a, b, dims, preferred_element_type=F32)


def call(kernel, outs, *args, scratch=(), flops=0, mib=24):
    place = {"v": pltpu.VMEM, "h": pltpu.HBM, "w": pltpu.HBM}
    spec = {"v": IN_VMEM, "w": IN_VMEM, "h": IN_HBM, "s": IN_SMEM}
    moved = sum(a.size * a.dtype.itemsize for a, _ in args)
    kernel_call = pl.pallas_call(
        kernel,
        out_shape=[place[m](shape, dtype) for shape, dtype, m in outs],
        in_specs=[spec[m] for _, m in args],
        out_specs=[spec[m] for _, _, m in outs],
        scratch_shapes=list(scratch),
        cost_estimate=pl.CostEstimate(flops=flops, bytes_accessed=moved, transcendentals=0),
        compiler_params=pltpu.CompilerParams(vmem_limit_bytes=mib * 1024 * 1024),
    )
    return kernel_call(
        *(a if m == "s" else pltpu.with_memory_space_constraint(a, place[m]) for a, m in args)
    )


def slots_of(core, routes, experts, half):
    top_k, rows = routes.shape
    expert = lax.broadcasted_iota(jnp.int32, (experts, rows), 0)
    hits = [routes[k : k + 1, :] == expert for k in range(top_k)]
    named = functools.reduce(jnp.logical_or, hits)
    before = lax.broadcasted_iota(jnp.int32, (rows, rows), 0) < lax.broadcasted_iota(
        jnp.int32, (rows, rows), 1
    )
    ones = lambda mask: jnp.where(mask, 1.0, 0.0).astype(BF16)
    count = dot(ones(named), ones(before), NN)
    slots = []
    for k in range(top_k):
        place = jnp.sum(jnp.where(hits[k], count, 0.0), axis=0, keepdims=True).astype(jnp.int32)
        place = place - core * half
        inside = (place >= 0) & (place < half)
        slots.append(jnp.where(inside, routes[k : k + 1, :] * half + place, -1))
    return slots


def masks_of(slots, count):
    row = lax.broadcasted_iota(jnp.int32, (count, slots[0].shape[1]), 0)
    return [row == s for s in slots]


def pick_of(masks):
    hit = functools.reduce(jnp.logical_or, masks)
    return jnp.where(hit, 1.0, 0.0).astype(BF16)


def send_tokens(experts, half, core_ref, par_ref, routes_ref, tok_ref, out_ref, tok, sem):
    copies = [
        pltpu.make_async_copy(tok_ref.at[:, cols], tok.at[:, to], sem.at[n])
        for n, (to, cols) in enumerate(side_columns(par_ref[0], tok_ref.shape[1]))
    ]
    for copy in copies:
        copy.start()
    masks = masks_of(slots_of(core_ref[0], routes_ref[...], experts, half), experts * half)
    for copy in copies:
        copy.wait()
    out_ref[...] = dot(pick_of(masks), tok[...], NN).astype(BF16)


def keep_table(experts, half, core_ref, routes_ref, gates_ref, out_ref):
    slots = slots_of(core_ref[0], routes_ref[...], experts, half)
    top_k = len(slots)
    gates = gates_ref[...].astype(F32)
    out_ref[...] = jnp.zeros(out_ref.shape, F32)
    for k in range(top_k):
        out_ref[k : k + 1] = slots[k].astype(F32)
        out_ref[top_k + k : top_k + k + 1] = gates[k : k + 1]


def table_slots(table_ref):
    return [table_ref[k : k + 1].astype(jnp.int32) for k in range(2)]


def send_cotangents(table_ref, cot_ref, out_ref):
    masks = masks_of(table_slots(table_ref), out_ref.shape[0])
    weigh = jnp.zeros(masks[0].shape, F32)
    for k, mask in enumerate(masks):
        weigh = jnp.where(mask, table_ref[2 + k : 3 + k], weigh)
    out_ref[...] = dot(weigh.astype(BF16), cot_ref[...], NN).astype(BF16)


def side_columns(side, width):
    step = width // 8
    return [
        (slice(m * step, (m + 1) * step), pl.ds(pl.multiple_of((2 * m + side) * step, step), step))
        for m in range(4)
    ]


def pack(par_ref, gate_ref, up_ref, out_ref, buf, sem, made, out_sem):
    copies = [pltpu.make_async_copy(w, buf.at[n], sem.at[n]) for n, w in enumerate((gate_ref, up_ref))]
    for copy in copies:
        copy.start()
    done = []
    for n, copy in enumerate(copies):
        copy.wait()
        for k in range(2):
            for to, cols in side_columns(jnp.where(k == 0, par_ref[0], 1 - par_ref[0]), buf.shape[2]):
                made[n, k, :, to] = buf[n, :, cols]
            done.append(pltpu.make_async_copy(made.at[n, k], out_ref.at[n, k], out_sem.at[2 * n + k]))
            done[-1].start()
    for copy in done:
        copy.wait()


def fetch_rows(low_ref, high_ref, both, sem):
    rows = low_ref.shape[0]
    copies = [
        pltpu.make_async_copy(low_ref, both.at[:rows], sem.at[0]),
        pltpu.make_async_copy(high_ref, both.at[rows:], sem.at[1]),
    ]
    for copy in copies:
        copy.start()
    return copies


def forward(mine_ref, low_ref, high_ref, own_ref, other_ref, out_ref, buf, sem, both, half_sem, made, out_sem):
    jobs = [(w.at[n, k], buf.at[2 * p + n, k]) for p, w in enumerate((own_ref, other_ref)) for n in range(2) for k in range(2)]
    copies = [pltpu.make_async_copy(a, b, sem.at[i]) for i, (a, b) in enumerate(jobs)]
    for copy in copies[:2]:
        copy.start()
    halves = fetch_rows(low_ref, high_ref, both, half_sem)
    for copy in copies[2:4]:
        copy.start()
    done = []

    def product(n):
        copies[2 * n].wait()
        copies[2 * n + 1].wait()
        for copy in copies[2 * n + 4 : 2 * n + 6]:
            copy.start()
        total = dot(mine_ref[...], buf[n, 0], NT)
        if n == 0:
            for copy in halves:
                copy.wait()
        return total + dot(both[...], buf[n, 1], NT)

    for p in range(2):
        pre = product(2 * p)
        up = product(2 * p + 1)
        sig = jax.nn.sigmoid(pre)
        act = pre * sig
        made[p, 0] = (act * up).astype(BF16)
        made[p, 1] = (up * sig * (1.0 + pre * (1.0 - sig))).astype(BF16)
        made[p, 2] = act.astype(BF16)
        done.append(pltpu.make_async_copy(made.at[p], out_ref.at[p], out_sem.at[p]))
        done[-1].start()
    for copy in done:
        copy.wait()


def input_grad(grads, buf):
    total = dot(grads[0, 0], buf[0], NN)
    total += dot(grads[0, 1], buf[1], NN)
    total += dot(grads[1, 0], buf[2], NN)
    return total + dot(grads[1, 1], buf[3], NN)


def fetch_half(k, own_ref, other_ref, buf, sem):
    return [
        pltpu.make_async_copy(w.at[n, k], buf.at[2 * p + n], sem.at[2 * p + n])
        for p, w in enumerate((own_ref, other_ref))
        for n in range(2)
    ]


def backward(cot_ref, mid_ref, down0_ref, down1_ref, own_ref, other_ref, low_ref, high_ref, grads_ref, gate_ref, mid, mid_sem, wd, wd_sem, buf, sem, grads, out_sem):
    rows, width = cot_ref.shape
    mids = [pltpu.make_async_copy(mid_ref.at[p], mid.at[p], mid_sem.at[p]) for p in range(2)]
    downs = [
        pltpu.make_async_copy(w, wd.at[p], wd_sem.at[p]) for p, w in enumerate((down0_ref, down1_ref))
    ]
    columns = fetch_half(1, own_ref, other_ref, buf, sem)
    downs[0].start()
    mids[0].start()
    downs[1].start()
    mids[1].start()
    gate = jnp.zeros((rows, 1), F32)
    done = []
    for p in range(2):
        downs[p].wait()
        for copy in columns[2 * p : 2 * p + 2]:
            copy.start()
        back = dot(cot_ref[...], wd[p], NT)
        mids[p].wait()
        gate = gate + jnp.sum(mid[p, 0].astype(F32) * back, axis=1, keepdims=True)
        grads[p, 0] = (back * mid[p, 1].astype(F32)).astype(BF16)
        grads[p, 1] = (back * mid[p, 2].astype(F32)).astype(BF16)
        done.append(pltpu.make_async_copy(grads.at[p], grads_ref.at[p], out_sem.at[p]))
        done[-1].start()
    wide = jnp.broadcast_to(gate, (rows, LANES))
    gate_ref[...] = wide
    low_ref[:, width // 2 :] = wide[: rows // 2].astype(BF16)
    high_ref[:, width // 2 :] = wide[rows // 2 :].astype(BF16)
    for copy in columns:
        copy.wait()
    total = input_grad(grads, buf).astype(BF16)
    low_ref[:, : width // 2] = total[: rows // 2]
    high_ref[:, : width // 2] = total[rows // 2 :]
    for copy in done:
        copy.wait()


def own_half(grads_ref, gate_ref, own_ref, other_ref, out_ref, grads, grad_sem, buf, sem):
    copies = [pltpu.make_async_copy(grads_ref.at[p], grads.at[p], grad_sem.at[p]) for p in range(2)]
    copies += fetch_half(0, own_ref, other_ref, buf, sem)
    for copy in copies:
        copy.start()
    part = buf.shape[2]
    out_ref[:, part:] = gate_ref[...]
    for copy in copies:
        copy.wait()
    out_ref[:, :part] = input_grad(grads, buf)


def add_pair(own_ref, low_ref, high_ref, out_ref):
    rows = low_ref.shape[0]
    out_ref[:rows] = (own_ref[:rows] + low_ref[...].astype(F32)).astype(BF16)
    out_ref[rows:] = (own_ref[rows:] + high_ref[...].astype(F32)).astype(BF16)


def weight_grads(p, par_ref, mine_ref, low_ref, high_ref, cot_ref, mid_ref, grads_ref, *refs):
    inputs = refs[:3] if p == 0 else ()
    outs, (both, half_sem, made, out_sem, left, left_sem, *got) = refs[len(inputs) :][:3], refs[len(inputs) + 3 :]
    lefts = [grads_ref.at[p, 0], grads_ref.at[p, 1], mid_ref.at[p, 0]]
    copies = [pltpu.make_async_copy(r, left.at[n], left_sem.at[n]) for n, r in enumerate(lefts)]
    received = [pltpu.make_async_copy(r, got[0].at[n], got[1].at[n]) for n, r in enumerate(inputs)]
    halves = fetch_rows(low_ref, high_ref, both, half_sem)
    for copy in copies + received:
        copy.start()
    done = []

    def put(n, cols, grad):
        if p == 0:
            grad += got[0][n, :, cols].astype(F32)
        made[n, :, cols] = grad.astype(BF16)

    for n in range(3):
        copies[n].wait()
        if p == 0:
            received[n].wait()
        if n == 0:
            for copy in halves:
                copy.wait()
        if n < 2:
            for side, right in ((par_ref[0], mine_ref), (1 - par_ref[0], both)):
                grad = dot(left[n], right[...], TN)
                for to, cols in side_columns(side, made.shape[2]):
                    put(n, cols, grad[:, to])
        else:
            put(n, slice(None), dot(left[n], cot_ref[...], TN))
        done.append(pltpu.make_async_copy(made.at[n], outs[n], out_sem.at[n]))
        done[-1].start()
    for copy in done:
        copy.wait()


def combine(core_ref, table_ref, x_ref, keep_ref, send_ref):
    blocks, padded, _ = keep_ref.shape
    rows = table_ref.shape[1]
    width = 2 * blocks * LANES
    core = core_ref[0]
    masks = masks_of(table_slots(table_ref), x_ref.shape[0])
    grads = dot(pick_of(masks), x_ref[:, :width], TN)
    gate = x_ref[:, width : width + 1].astype(F32)
    lines = []
    for mask in masks:
        line = jnp.sum(jnp.where(mask, gate, 0.0), axis=0, keepdims=True)
        line = jnp.concatenate([line, jnp.zeros((1, 2 * LANES - rows), F32)], axis=1)
        lines += [line[:, :LANES], line[:, LANES:]]
    lines.append(jnp.zeros((padded - rows - len(lines), LANES), F32))
    tail = jnp.concatenate(lines, axis=0)
    for b in range(blocks):
        first = grads[:, 2 * b * LANES : (2 * b + 1) * LANES]
        second = grads[:, (2 * b + 1) * LANES : (2 * b + 2) * LANES]
        keep_ref[b, :rows, :] = jnp.where(core == 0, first, second)
        send_ref[b, :rows, :] = jnp.where(core == 0, second, first).astype(BF16)
        keep_ref[b, rows:, :] = tail
        send_ref[b, rows:, :] = tail.astype(BF16)


def join(turn_ref, keep_ref, got_ref, *out_refs):
    for k, out_ref in enumerate(out_refs):
        block = lax.rem(turn_ref[0] + k, len(out_refs))
        out_ref[...] = (keep_ref[block] + got_ref[block].astype(F32)).astype(BF16)


def finish(table_ref, *refs):
    parts, (tok_ref, gate_ref) = refs[:-2], refs[-2:]
    top_k, rows = gate_ref.shape
    total = functools.reduce(jnp.add, [x[...].astype(F32) for x in parts])
    tok_ref[...] = total[:rows].astype(BF16)
    for k in range(top_k):
        line = jnp.concatenate(
            [total[rows + 2 * k : rows + 2 * k + 1], total[rows + 2 * k + 1 : rows + 2 * k + 2]],
            axis=1,
        )
        gate_ref[k : k + 1, :] = line[:, :rows] / table_ref[top_k + k : top_k + k + 1, :]


def local(experts, tokens, cotangent, routing, gate_weights, gate_proj, up_proj, down_proj):
    rows, width = tokens.shape
    top_k = routing.shape[1]
    half = rows * top_k // experts
    count = experts * half
    part = width // 2
    depth = lax.axis_size(Z)
    core = lax.axis_index("c").astype(jnp.int32).reshape(1)
    parity = (lax.axis_index(Z) % 2).astype(jnp.int32).reshape(1)
    routes, gates = routing.T, gate_weights.T

    def swap(v):
        return lax.ppermute(v, "c", [(0, 1), (1, 0)])

    def shift(v, k):
        return lax.ppermute(v, Z, [(i, (i + k) % depth) for i in range(depth)])

    def exchange(v):
        return lax.all_to_all(v, EP, split_axis=0, concat_axis=0, tiled=True)

    dma = lambda n: pltpu.SemaphoreType.DMA((n,))

    ff = gate_proj.shape[2]
    down = down_proj[0]
    down_other = swap(down)
    (own,) = call(
        pack, [((2, 2, ff, part), BF16, "h")],
        (parity, "s"), (gate_proj[0].T, "h"), (up_proj[0].T, "h"),
        scratch=[
            pltpu.VMEM((2, ff, width), BF16), dma(2), pltpu.VMEM((2, 2, ff, part), BF16), dma(4),
        ],
        mib=10,
    )
    other = swap(own)
    (table,) = call(
        functools.partial(keep_table, experts, half), [((8, rows), F32, "v")],
        (core, "s"), (routes, "w"), (gates, "w"), mib=4,
    )

    (tok_out,) = call(
        functools.partial(send_tokens, experts, half),
        [((count, part), BF16, "w")],
        (core, "s"), (parity, "s"), (routes, "w"), (tokens, "h"),
        scratch=[pltpu.VMEM((rows, part), BF16), dma(4)],
        flops=2 * count * rows * part, mib=8,
    )
    mine = exchange(tok_out.reshape(experts, half, part)).reshape(count, part)
    (cot_out,) = call(
        send_cotangents, [((count, width), BF16, "w")],
        (table, "v"), (cotangent, "w"),
        flops=2 * count * rows * width, mib=8,
    )
    cot = exchange(cot_out.reshape(experts, half, width)).reshape(count, width)
    low = shift(mine[: count // 2], 1)
    high = shift(mine[count // 2 :], -1)

    packed = [(own, "h"), (other, "h")]
    mids = pltpu.VMEM((2, 3, count, ff), BF16)
    halves = [pltpu.VMEM((4, ff, part), BF16), dma(4)]
    (mid,) = call(
        forward, [((2, 3, count, ff), BF16, "h")],
        (mine, "v"), (low, "h"), (high, "h"), *packed,
        scratch=[
            pltpu.VMEM((4, 2, ff, part), BF16), dma(8), pltpu.VMEM((count, part), BF16), dma(2), mids, dma(2),
        ],
        flops=8 * count * width * ff, mib=18,
    )
    message = ((count // 2, part + LANES), BF16, "v")
    to_low, to_high, grads, gate = call(
        backward,
        [message, message, ((2, 2, count, ff), BF16, "h"), ((count, LANES), F32, "v")],
        (cot, "v"), (mid, "h"), (down, "h"), (down_other, "h"), *packed,
        scratch=[
            mids, dma(2), pltpu.VMEM((2, ff, width), BF16), dma(2), *halves,
            pltpu.VMEM((2, 2, count, ff), BF16), dma(2),
        ],
        flops=8 * count * width * ff, mib=20,
    )
    from_low, from_high = shift(to_low, -1), shift(to_high, 1)
    (kept,) = call(
        own_half, [((count, part + LANES), F32, "v")],
        (grads, "h"), (gate, "v"), *packed,
        scratch=[pltpu.VMEM((2, 2, count, ff), BF16), dma(2), *halves],
        flops=4 * count * width * ff, mib=14,
    )
    (pair,) = call(
        add_pair, [((count, part + LANES), BF16, "w")], (kept, "v"), (from_low, "v"), (from_high, "v"), mib=8
    )
    returned = exchange(pair.reshape(experts, half, part + LANES)).reshape(count, part + LANES)

    pieces = [(mine, "v"), (low, "h"), (high, "h"), (cot, "v"), (mid, "h"), (grads, "h")]
    shard = [((ff, width), BF16, "h")] * 3
    whole = pltpu.VMEM((3, ff, width), BF16)
    room = [pltpu.VMEM((count, part), BF16), dma(2), whole, dma(3), pltpu.VMEM((3, count, ff), BF16), dma(3)]
    theirs = call(
        functools.partial(weight_grads, 1), shard, (parity, "s"), *pieces,
        scratch=room, flops=6 * count * width * ff, mib=14,
    )
    received = [(swap(g), "h") for g in theirs]
    grad_gate, grad_up, grad_down = call(
        functools.partial(weight_grads, 0), shard, (parity, "s"), *pieces, *received,
        scratch=[*room, whole, dma(3)], flops=6 * count * width * ff, mib=20,
    )

    block = (depth // 2, rows + 16, LANES)
    keep, send = call(
        combine, [(block, F32, "v"), (block, BF16, "v")],
        (core, "s"), (table, "v"), (returned, "v"),
        flops=2 * count * rows * part, mib=10,
    )
    turn = lax.axis_index("zh").astype(jnp.int32).reshape(1)
    steps = depth // 2
    parts = call(
        join, [(block[1:], BF16, "v")] * steps,
        (turn, "s"), (keep, "v"), (swap(send), "v"), mib=4,
    )
    sums = [parts[0]] + [shift(parts[k], 2 * k) for k in range(1, steps)]
    grad_tokens, grad_gates = call(
        finish,
        [((rows, LANES), BF16, "w"), ((top_k, rows), F32, "w")],
        (table, "v"), *((v, "v") for v in sums), mib=4,
    )
    return (grad_tokens, grad_gates.T, grad_gate.T[None], grad_up.T[None], grad_down[None])


def solution(mesh):
    devices = mesh.devices.reshape(4, 4, 4, 2, 2)
    inner = jax.sharding.Mesh(devices, (*EP, *Z, "c"))
    ep, tp = EP, (*Z, "c")

    def body(*args):
        return local(16, *args)

    return jax.shard_map(
        body,
        mesh=inner,
        in_specs=(
            P(ep, None),
            P(ep, None),
            P(ep, None),
            P(ep, None),
            P(ep, None, tp),
            P(ep, None, tp),
            P(ep, tp, None),
        ),
        out_specs=(
            P(ep, tp),
            P(ep, None),
            P(ep, None, tp),
            P(ep, None, tp),
            P(ep, tp, None),
        ),
        check_vma=False,
    )
```

```python
import functools

import jax
import jax.numpy as jnp
from jax import lax
from jax.experimental import pallas as pl
from jax.experimental.pallas import tpu as pltpu
from jax.sharding import PartitionSpec as P


EP = ("y", "x")
Z = ("zh", "zl")
LANES = 128
BF16 = jnp.bfloat16
F32 = jnp.float32
NN = (((1,), (0,)), ((), ()))
NT = (((1,), (1,)), ((), ()))
TN = (((0,), (0,)), ((), ()))
IN_VMEM = pl.BlockSpec(memory_space=pltpu.VMEM)
IN_HBM = pl.BlockSpec(memory_space=pltpu.HBM)
IN_SMEM = pl.BlockSpec(memory_space=pltpu.SMEM)


def dot(a, b, dims):
    return lax.dot_general(a, b, dims, preferred_element_type=F32)


def call(kernel, outs, *args, scratch=(), flops=0, mib=24):
    place = {"v": pltpu.VMEM, "h": pltpu.HBM, "w": pltpu.HBM}
    spec = {"v": IN_VMEM, "w": IN_VMEM, "h": IN_HBM, "s": IN_SMEM}
    moved = sum(a.size * a.dtype.itemsize for a, _ in args)
    kernel_call = pl.pallas_call(
        kernel,
        out_shape=[place[m](shape, dtype) for shape, dtype, m in outs],
        in_specs=[spec[m] for _, m in args],
        out_specs=[spec[m] for _, _, m in outs],
        scratch_shapes=list(scratch),
        cost_estimate=pl.CostEstimate(flops=flops, bytes_accessed=moved, transcendentals=0),
        compiler_params=pltpu.CompilerParams(vmem_limit_bytes=mib * 1024 * 1024),
    )
    return kernel_call(
        *(a if m == "s" else pltpu.with_memory_space_constraint(a, place[m]) for a, m in args)
    )


def slots_of(core, routes, experts, half):
    top_k, rows = routes.shape
    expert = lax.broadcasted_iota(jnp.int32, (experts, rows), 0)
    hits = [routes[k : k + 1, :] == expert for k in range(top_k)]
    named = functools.reduce(jnp.logical_or, hits)
    before = lax.broadcasted_iota(jnp.int32, (rows, rows), 0) < lax.broadcasted_iota(
        jnp.int32, (rows, rows), 1
    )
    ones = lambda mask: jnp.where(mask, 1.0, 0.0).astype(BF16)
    count = dot(ones(named), ones(before), NN)
    slots = []
    for k in range(top_k):
        place = jnp.sum(jnp.where(hits[k], count, 0.0), axis=0, keepdims=True).astype(jnp.int32)
        place = place - core * half
        inside = (place >= 0) & (place < half)
        slots.append(jnp.where(inside, routes[k : k + 1, :] * half + place, -1))
    return slots


def masks_of(slots, count):
    row = lax.broadcasted_iota(jnp.int32, (count, slots[0].shape[1]), 0)
    return [row == s for s in slots]


def pick_of(masks):
    hit = functools.reduce(jnp.logical_or, masks)
    return jnp.where(hit, 1.0, 0.0).astype(BF16)


def send_tokens(experts, half, core_ref, par_ref, routes_ref, tok_ref, out_ref, routes, route_sem, tok, sem, made, out_sem):
    route = pltpu.make_async_copy(routes_ref, routes, route_sem)
    route.start()
    copies = [
        pltpu.make_async_copy(tok_ref.at[:, cols], tok.at[:, to], sem.at[n])
        for n, (to, cols) in enumerate(side_columns(par_ref[0], tok_ref.shape[1]))
    ]
    for copy in copies:
        copy.start()
    route.wait()
    masks = masks_of(slots_of(core_ref[0], routes[...], experts, half), experts * half)
    for copy in copies:
        copy.wait()
    pick = pick_of(masks)
    part = out_ref.shape[1]
    done = []
    for n in range(2):
        cols = slice(n * part // 2, (n + 1) * part // 2)
        made[:, cols] = dot(pick, tok[:, cols], NN).astype(BF16)
        done.append(pltpu.make_async_copy(made.at[:, cols], out_ref.at[:, cols], out_sem.at[n]))
        done[-1].start()
    for copy in done:
        copy.wait()


def keep_table(experts, half, core_ref, routes_ref, gates_ref, out_ref):
    slots = slots_of(core_ref[0], routes_ref[...], experts, half)
    top_k = len(slots)
    gates = gates_ref[...].astype(F32)
    out_ref[...] = jnp.zeros(out_ref.shape, F32)
    for k in range(top_k):
        out_ref[k : k + 1] = slots[k].astype(F32)
        out_ref[top_k + k : top_k + k + 1] = gates[k : k + 1]


def table_slots(table_ref):
    return [table_ref[k : k + 1].astype(jnp.int32) for k in range(2)]


def send_cotangents(table_ref, cot_ref, out_ref):
    masks = masks_of(table_slots(table_ref), out_ref.shape[0])
    weigh = jnp.zeros(masks[0].shape, F32)
    for k, mask in enumerate(masks):
        weigh = jnp.where(mask, table_ref[2 + k : 3 + k], weigh)
    out_ref[...] = dot(weigh.astype(BF16), cot_ref[...], NN).astype(BF16)


def side_columns(side, width):
    step = width // 8
    return [
        (slice(m * step, (m + 1) * step), pl.ds(pl.multiple_of((2 * m + side) * step, step), step))
        for m in range(4)
    ]


def pack(par_ref, gate_ref, up_ref, out_ref, buf, sem, made, out_sem):
    copies = [pltpu.make_async_copy(w, buf.at[n], sem.at[n]) for n, w in enumerate((gate_ref, up_ref))]
    for copy in copies:
        copy.start()
    done = []
    for n, copy in enumerate(copies):
        copy.wait()
        for k in range(2):
            for to, cols in side_columns(jnp.where(k == 0, par_ref[0], 1 - par_ref[0]), buf.shape[2]):
                made[n, k, :, to] = buf[n, :, cols]
            done.append(pltpu.make_async_copy(made.at[n, k], out_ref.at[n, k], out_sem.at[2 * n + k]))
            done[-1].start()
    for copy in done:
        copy.wait()


def forward(mine_ref, low_ref, high_ref, own_ref, other_ref, out_ref, both_ref, buf, sem, both, both_sem, made, out_sem):
    jobs = [(w.at[n, k], buf.at[2 * p + n, k]) for p, w in enumerate((own_ref, other_ref)) for n in range(2) for k in range(2)]
    copies = [pltpu.make_async_copy(a, b, sem.at[i]) for i, (a, b) in enumerate(jobs)]
    for copy in copies:
        copy.start()
    rows = low_ref.shape[0]
    both[:rows] = low_ref[...]
    both[rows:] = high_ref[...]
    keep = pltpu.make_async_copy(both, both_ref, both_sem)
    keep.start()
    done = []

    def product(n):
        copies[2 * n].wait()
        copies[2 * n + 1].wait()
        return dot(mine_ref[...], buf[n, 0], NT) + dot(both[...], buf[n, 1], NT)

    for p in range(2):
        pre = product(2 * p)
        up = product(2 * p + 1)
        sig = jax.nn.sigmoid(pre)
        act = pre * sig
        made[p, 0] = (act * up).astype(BF16)
        made[p, 1] = (up * sig * (1.0 + pre * (1.0 - sig))).astype(BF16)
        made[p, 2] = act.astype(BF16)
        done.append(pltpu.make_async_copy(made.at[p], out_ref.at[p], out_sem.at[p]))
        done[-1].start()
    for copy in [keep, *done]:
        copy.wait()


def input_grad(grads, buf):
    total = dot(grads[0, 0], buf[0], NN)
    total += dot(grads[0, 1], buf[1], NN)
    total += dot(grads[1, 0], buf[2], NN)
    return total + dot(grads[1, 1], buf[3], NN)


def fetch_half(k, own_ref, other_ref, buf, sem):
    return [
        pltpu.make_async_copy(w.at[n, k], buf.at[2 * p + n], sem.at[2 * p + n])
        for p, w in enumerate((own_ref, other_ref))
        for n in range(2)
    ]


def backward(cot_ref, mid_ref, down0_ref, down1_ref, own_ref, other_ref, low_ref, high_ref, grads_ref, gate_ref, mid, mid_sem, wd, wd_sem, buf, sem, grads, out_sem):
    rows, width = cot_ref.shape
    mids = [pltpu.make_async_copy(mid_ref.at[p], mid.at[p], mid_sem.at[p]) for p in range(2)]
    downs = [
        pltpu.make_async_copy(w, wd.at[p], wd_sem.at[p]) for p, w in enumerate((down0_ref, down1_ref))
    ]
    columns = fetch_half(1, own_ref, other_ref, buf, sem)
    for copy in (downs[0], mids[0], downs[1], mids[1], *columns):
        copy.start()
    gate = jnp.zeros((rows, 1), F32)
    done = []
    for p in range(2):
        downs[p].wait()
        back = dot(cot_ref[...], wd[p], NT)
        mids[p].wait()
        gate = gate + jnp.sum(mid[p, 0].astype(F32) * back, axis=1, keepdims=True)
        grads[p, 0] = (back * mid[p, 1].astype(F32)).astype(BF16)
        grads[p, 1] = (back * mid[p, 2].astype(F32)).astype(BF16)
        done.append(pltpu.make_async_copy(grads.at[p], grads_ref.at[p], out_sem.at[p]))
        done[-1].start()
    wide = jnp.broadcast_to(gate, (rows, LANES))
    gate_ref[...] = wide
    low_ref[:, width // 2 :] = wide[: rows // 2].astype(BF16)
    high_ref[:, width // 2 :] = wide[rows // 2 :].astype(BF16)
    for copy in columns:
        copy.wait()
    total = input_grad(grads, buf).astype(BF16)
    low_ref[:, : width // 2] = total[: rows // 2]
    high_ref[:, : width // 2] = total[rows // 2 :]
    for copy in done:
        copy.wait()


def own_half(grads_ref, gate_ref, own_ref, other_ref, out_ref, grads, grad_sem, buf, sem):
    copies = [pltpu.make_async_copy(grads_ref.at[p], grads.at[p], grad_sem.at[p]) for p in range(2)]
    copies += fetch_half(0, own_ref, other_ref, buf, sem)
    for copy in copies:
        copy.start()
    part = buf.shape[2]
    out_ref[:, part:] = gate_ref[...]
    for copy in copies:
        copy.wait()
    out_ref[:, :part] = input_grad(grads, buf)


def add_pair(own_ref, low_ref, high_ref, out_ref, made, sem):
    rows = low_ref.shape[0]
    done = []
    for n, other in enumerate((low_ref, high_ref)):
        span = slice(n * rows, (n + 1) * rows)
        made[span] = (own_ref[span] + other[...].astype(F32)).astype(BF16)
        done.append(pltpu.make_async_copy(made.at[span], out_ref.at[span], sem.at[n]))
        done[-1].start()
    for copy in done:
        copy.wait()


def row_grads(p, par_ref, mine_ref, both_ref, grads_ref, *refs):
    inputs = refs[:2] if p == 0 else ()
    outs, scratch = refs[len(inputs) : len(inputs) + 2], refs[len(inputs) + 2 :]
    both, both_sem, left, left_sem, made, out_sem, *got = scratch
    keep = pltpu.make_async_copy(both_ref, both, both_sem)
    copies = [pltpu.make_async_copy(grads_ref.at[p, n], left.at[n], left_sem.at[n]) for n in range(2)]
    received = [pltpu.make_async_copy(r, got[0].at[n], got[1].at[n]) for n, r in enumerate(inputs)]
    for copy in (copies[0], keep, copies[1], *received):
        copy.start()
    done = []
    for n in range(2):
        copies[n].wait()
        if p == 0:
            received[n].wait()
        for side, right in ((par_ref[0], mine_ref), (1 - par_ref[0], both)):
            if n == 0 and right is both:
                keep.wait()
            grad = dot(left[n], right[...], TN)
            for to, cols in side_columns(side, made.shape[2]):
                piece = grad[:, to]
                if p == 0:
                    piece = piece + got[0][n, :, cols].astype(F32)
                made[n, :, cols] = piece.astype(BF16)
        done.append(pltpu.make_async_copy(made.at[n], outs[n], out_sem.at[n]))
        done[-1].start()
    for copy in done:
        copy.wait()


def down_grads(p, cot_ref, mid_ref, *refs):
    inputs, (out_ref, left, sem, made, out_sem, *got) = (refs[:1], refs[1:]) if p == 0 else ((), refs)
    copies = [pltpu.make_async_copy(mid_ref.at[p, 0], left, sem)]
    copies += [pltpu.make_async_copy(r, got[0], got[1]) for r in inputs]
    for copy in copies:
        copy.start()
    for copy in copies:
        copy.wait()
    grad = dot(left[...], cot_ref[...], TN)
    if p == 0:
        grad += got[0][...].astype(F32)
    made[...] = grad.astype(BF16)
    done = pltpu.make_async_copy(made, out_ref, out_sem)
    done.start()
    done.wait()


def combine(core_ref, table_ref, x_ref, keep_ref, send_ref):
    blocks, padded, _ = keep_ref.shape
    rows = table_ref.shape[1]
    width = 2 * blocks * LANES
    core = core_ref[0]
    masks = masks_of(table_slots(table_ref), x_ref.shape[0])
    grads = dot(pick_of(masks), x_ref[:, :width], TN)
    gate = x_ref[:, width : width + 1].astype(F32)
    lines = []
    for mask in masks:
        line = jnp.sum(jnp.where(mask, gate, 0.0), axis=0, keepdims=True)
        line = jnp.concatenate([line, jnp.zeros((1, 2 * LANES - rows), F32)], axis=1)
        lines += [line[:, :LANES], line[:, LANES:]]
    lines.append(jnp.zeros((padded - rows - len(lines), LANES), F32))
    tail = jnp.concatenate(lines, axis=0)
    for b in range(blocks):
        first = grads[:, 2 * b * LANES : (2 * b + 1) * LANES]
        second = grads[:, (2 * b + 1) * LANES : (2 * b + 2) * LANES]
        keep_ref[b, :rows, :] = jnp.where(core == 0, first, second)
        send_ref[b, :rows, :] = jnp.where(core == 0, second, first).astype(BF16)
        keep_ref[b, rows:, :] = tail
        send_ref[b, rows:, :] = tail.astype(BF16)


def join(turn_ref, keep_ref, got_ref, *out_refs):
    for k, out_ref in enumerate(out_refs):
        block = lax.rem(turn_ref[0] + k, len(out_refs))
        out_ref[...] = (keep_ref[block] + got_ref[block].astype(F32)).astype(BF16)


def finish(table_ref, *refs):
    parts, (tok_ref, gate_ref) = refs[:-2], refs[-2:]
    top_k, rows = gate_ref.shape
    total = functools.reduce(jnp.add, [x[...].astype(F32) for x in parts])
    tok_ref[...] = total[:rows].astype(BF16)
    for k in range(top_k):
        line = jnp.concatenate(
            [total[rows + 2 * k : rows + 2 * k + 1], total[rows + 2 * k + 1 : rows + 2 * k + 2]],
            axis=1,
        )
        gate_ref[k : k + 1, :] = line[:, :rows] / table_ref[top_k + k : top_k + k + 1, :]


def local(experts, tokens, cotangent, routing, gate_weights, gate_proj, up_proj, down_proj):
    rows, width = tokens.shape
    top_k = routing.shape[1]
    half = rows * top_k // experts
    count = experts * half
    part = width // 2
    depth = lax.axis_size(Z)
    core = lax.axis_index("c").astype(jnp.int32).reshape(1)
    parity = (lax.axis_index(Z) % 2).astype(jnp.int32).reshape(1)
    routes, gates = routing.T, gate_weights.T

    def swap(v):
        return lax.ppermute(v, "c", [(0, 1), (1, 0)])

    def shift(v, k):
        return lax.ppermute(v, Z, [(i, (i + k) % depth) for i in range(depth)])

    def exchange(v):
        return lax.all_to_all(v, EP, split_axis=0, concat_axis=0, tiled=True)

    dma = lambda n: pltpu.SemaphoreType.DMA((n,))

    ff = gate_proj.shape[2]
    down = down_proj[0]
    down_other = swap(down)
    (own,) = call(
        pack, [((2, 2, ff, part), BF16, "h")],
        (parity, "s"), (gate_proj[0].T, "h"), (up_proj[0].T, "h"),
        scratch=[
            pltpu.VMEM((2, ff, width), BF16), dma(2), pltpu.VMEM((2, 2, ff, part), BF16), dma(4),
        ],
        mib=10,
    )
    other = swap(own)
    (table,) = call(
        functools.partial(keep_table, experts, half), [((8, rows), F32, "v")],
        (core, "s"), (routes, "w"), (gates, "w"), mib=4,
    )

    (tok_out,) = call(
        functools.partial(send_tokens, experts, half),
        [((count, part), BF16, "h")],
        (core, "s"), (parity, "s"), (routes, "h"), (tokens, "h"),
        scratch=[
            pltpu.VMEM((top_k, rows), jnp.int32), pltpu.SemaphoreType.DMA,
            pltpu.VMEM((rows, part), BF16), dma(4), pltpu.VMEM((count, part), BF16), dma(2),
        ],
        flops=2 * count * rows * part, mib=8,
    )
    mine = exchange(tok_out.reshape(experts, half, part)).reshape(count, part)
    (cot_out,) = call(
        send_cotangents, [((count, width), BF16, "w")],
        (table, "v"), (cotangent, "w"),
        flops=2 * count * rows * width, mib=8,
    )
    cot = exchange(cot_out.reshape(experts, half, width)).reshape(count, width)
    low = shift(mine[: count // 2], 1)
    high = shift(mine[count // 2 :], -1)

    packed = [(own, "h"), (other, "h")]
    mids = pltpu.VMEM((2, 3, count, ff), BF16)
    halves = [pltpu.VMEM((4, ff, part), BF16), dma(4)]
    mid, both = call(
        forward, [((2, 3, count, ff), BF16, "h"), ((count, part), BF16, "h")],
        (mine, "v"), (low, "v"), (high, "v"), *packed,
        scratch=[
            pltpu.VMEM((4, 2, ff, part), BF16), dma(8), pltpu.VMEM((count, part), BF16),
            pltpu.SemaphoreType.DMA, mids, dma(2),
        ],
        flops=8 * count * width * ff, mib=18,
    )
    message = ((count // 2, part + LANES), BF16, "v")
    to_low, to_high, grads, gate = call(
        backward,
        [message, message, ((2, 2, count, ff), BF16, "h"), ((count, LANES), F32, "v")],
        (cot, "v"), (mid, "h"), (down, "h"), (down_other, "h"), *packed,
        scratch=[
            mids, dma(2), pltpu.VMEM((2, ff, width), BF16), dma(2), *halves,
            pltpu.VMEM((2, 2, count, ff), BF16), dma(2),
        ],
        flops=8 * count * width * ff, mib=20,
    )
    from_low, from_high = shift(to_low, -1), shift(to_high, 1)
    (kept,) = call(
        own_half, [((count, part + LANES), F32, "v")],
        (grads, "h"), (gate, "v"), *packed,
        scratch=[pltpu.VMEM((2, 2, count, ff), BF16), dma(2), *halves],
        flops=4 * count * width * ff, mib=14,
    )
    (pair,) = call(
        add_pair, [((count, part + LANES), BF16, "h")], (kept, "v"), (from_low, "v"), (from_high, "v"),
        scratch=[pltpu.VMEM((count, part + LANES), BF16), dma(2)], mib=8,
    )
    returned = exchange(pair.reshape(experts, half, part + LANES)).reshape(count, part + LANES)

    one = pltpu.SemaphoreType.DMA
    shard = ((ff, width), BF16, "h")
    pair_room = pltpu.VMEM((2, ff, width), BF16)
    row_args = [(parity, "s"), (mine, "v"), (both, "h"), (grads, "h")]
    row_room = [
        pltpu.VMEM((count, part), BF16), one, pltpu.VMEM((2, count, ff), BF16), dma(2), pair_room, dma(2),
    ]
    down_args = [(cot, "v"), (mid, "h")]
    down_room = [pltpu.VMEM((count, ff), BF16), one, pltpu.VMEM((ff, width), BF16), one]
    cost = 2 * count * width * ff
    (their_down,) = call(
        functools.partial(down_grads, 1), [shard], *down_args,
        scratch=down_room, flops=cost, mib=10,
    )
    theirs = call(
        functools.partial(row_grads, 1), [shard] * 2, *row_args,
        scratch=row_room, flops=2 * cost, mib=14,
    )
    (grad_down,) = call(
        functools.partial(down_grads, 0), [shard], *down_args, (swap(their_down), "h"),
        scratch=[*down_room, down_room[2], one], flops=cost, mib=12,
    )
    received = [(swap(g), "h") for g in theirs]
    grad_gate, grad_up = call(
        functools.partial(row_grads, 0), [shard] * 2, *row_args, *received,
        scratch=[*row_room, pair_room, dma(2)], flops=2 * cost, mib=18,
    )

    block = (depth // 2, rows + 16, LANES)
    keep, send = call(
        combine, [(block, F32, "v"), (block, BF16, "v")],
        (core, "s"), (table, "v"), (returned, "v"),
        flops=2 * count * rows * part, mib=10,
    )
    turn = lax.axis_index("zh").astype(jnp.int32).reshape(1)
    steps = depth // 2
    parts = call(
        join, [(block[1:], BF16, "v")] * steps,
        (turn, "s"), (keep, "v"), (swap(send), "v"), mib=4,
    )
    sums = [parts[0]] + [shift(parts[k], 2 * k) for k in range(1, steps)]
    grad_tokens, grad_gates = call(
        finish,
        [((rows, LANES), BF16, "w"), ((top_k, rows), F32, "w")],
        (table, "v"), *((v, "v") for v in sums), mib=4,
    )
    return (grad_tokens, grad_gates.T, grad_gate.T[None], grad_up.T[None], grad_down[None])


def solution(mesh):
    devices = mesh.devices.reshape(4, 4, 4, 2, 2)
    inner = jax.sharding.Mesh(devices, (*EP, *Z, "c"))
    ep, tp = EP, (*Z, "c")

    def body(*args):
        return local(16, *args)

    return jax.shard_map(
        body,
        mesh=inner,
        in_specs=(
            P(ep, None),
            P(ep, None),
            P(ep, None),
            P(ep, None),
            P(ep, None, tp),
            P(ep, None, tp),
            P(ep, tp, None),
        ),
        out_specs=(
            P(ep, tp),
            P(ep, None),
            P(ep, None, tp),
            P(ep, None, tp),
            P(ep, tp, None),
        ),
        check_vma=False,
    )
```

```python
import functools

import jax
import jax.numpy as jnp
from jax import lax
from jax.experimental import pallas as pl
from jax.experimental.pallas import tpu as pltpu
from jax.sharding import PartitionSpec as P


EP = ("y", "x")
Z = ("zh", "zl")
LANES = 128
BF16 = jnp.bfloat16
F32 = jnp.float32
NN = (((1,), (0,)), ((), ()))
NT = (((1,), (1,)), ((), ()))
TN = (((0,), (0,)), ((), ()))
IN_VMEM = pl.BlockSpec(memory_space=pltpu.VMEM)
IN_HBM = pl.BlockSpec(memory_space=pltpu.HBM)
IN_SMEM = pl.BlockSpec(memory_space=pltpu.SMEM)


def dot(a, b, dims):
    return lax.dot_general(a, b, dims, preferred_element_type=F32)


def call(kernel, outs, *args, scratch=(), flops=0, mib=24):
    place = {"v": pltpu.VMEM, "h": pltpu.HBM, "w": pltpu.HBM}
    spec = {"v": IN_VMEM, "w": IN_VMEM, "h": IN_HBM, "s": IN_SMEM}
    moved = sum(a.size * a.dtype.itemsize for a, _ in args)
    kernel_call = pl.pallas_call(
        kernel,
        out_shape=[place[m](shape, dtype) for shape, dtype, m in outs],
        in_specs=[spec[m] for _, m in args],
        out_specs=[spec[m] for _, _, m in outs],
        scratch_shapes=list(scratch),
        cost_estimate=pl.CostEstimate(flops=flops, bytes_accessed=moved, transcendentals=0),
        compiler_params=pltpu.CompilerParams(vmem_limit_bytes=mib * 1024 * 1024),
    )
    return kernel_call(
        *(a if m == "s" else pltpu.with_memory_space_constraint(a, place[m]) for a, m in args)
    )


def slots_of(core, routes, experts, half):
    top_k, rows = routes.shape
    expert = lax.broadcasted_iota(jnp.int32, (experts, rows), 0)
    hits = [routes[k : k + 1, :] == expert for k in range(top_k)]
    named = functools.reduce(jnp.logical_or, hits)
    before = lax.broadcasted_iota(jnp.int32, (rows, rows), 0) < lax.broadcasted_iota(
        jnp.int32, (rows, rows), 1
    )
    ones = lambda mask: jnp.where(mask, 1.0, 0.0).astype(BF16)
    count = dot(ones(named), ones(before), NN)
    slots = []
    for k in range(top_k):
        place = jnp.sum(jnp.where(hits[k], count, 0.0), axis=0, keepdims=True).astype(jnp.int32)
        place = place - core * half
        inside = (place >= 0) & (place < half)
        slots.append(jnp.where(inside, routes[k : k + 1, :] * half + place, -1))
    return slots


def masks_of(slots, count):
    row = lax.broadcasted_iota(jnp.int32, (count, slots[0].shape[1]), 0)
    return [row == s for s in slots]


def pick_of(masks):
    hit = functools.reduce(jnp.logical_or, masks)
    return jnp.where(hit, 1.0, 0.0).astype(BF16)


def send_tokens(experts, half, core_ref, par_ref, routes_ref, tok_ref, out_ref, routes, route_sem, tok, sem, made, out_sem):
    route = pltpu.make_async_copy(routes_ref, routes, route_sem)
    route.start()
    copies = [
        pltpu.make_async_copy(tok_ref.at[:, cols], tok.at[:, to], sem.at[n])
        for n, (to, cols) in enumerate(side_columns(par_ref[0], tok_ref.shape[1]))
    ]
    for copy in copies:
        copy.start()
    route.wait()
    masks = masks_of(slots_of(core_ref[0], routes[...], experts, half), experts * half)
    for copy in copies:
        copy.wait()
    pick = pick_of(masks)
    part = out_ref.shape[1]
    done = []
    for n in range(2):
        cols = slice(n * part // 2, (n + 1) * part // 2)
        made[:, cols] = dot(pick, tok[:, cols], NN).astype(BF16)
        done.append(pltpu.make_async_copy(made.at[:, cols], out_ref.at[:, cols], out_sem.at[n]))
        done[-1].start()
    for copy in done:
        copy.wait()


def keep_table(experts, half, core_ref, routes_ref, gates_ref, out_ref):
    slots = slots_of(core_ref[0], routes_ref[...], experts, half)
    top_k = len(slots)
    gates = gates_ref[...].astype(F32)
    out_ref[...] = jnp.zeros(out_ref.shape, F32)
    for k in range(top_k):
        out_ref[k : k + 1] = slots[k].astype(F32)
        out_ref[top_k + k : top_k + k + 1] = gates[k : k + 1]


def table_slots(table_ref):
    return [table_ref[k : k + 1].astype(jnp.int32) for k in range(2)]


def send_cotangents(table_ref, cot_ref, out_ref):
    masks = masks_of(table_slots(table_ref), out_ref.shape[0])
    weigh = jnp.zeros(masks[0].shape, F32)
    for k, mask in enumerate(masks):
        weigh = jnp.where(mask, table_ref[2 + k : 3 + k], weigh)
    out_ref[...] = dot(weigh.astype(BF16), cot_ref[...], NN).astype(BF16)


def side_columns(side, width):
    step = width // 8
    return [
        (slice(m * step, (m + 1) * step), pl.ds(pl.multiple_of((2 * m + side) * step, step), step))
        for m in range(4)
    ]


def pack(par_ref, gate_ref, up_ref, out_ref, buf, sem, made, out_sem):
    copies = [pltpu.make_async_copy(w, buf.at[n], sem.at[n]) for n, w in enumerate((gate_ref, up_ref))]
    for copy in copies:
        copy.start()
    done = []
    for n, copy in enumerate(copies):
        copy.wait()
        for k in range(2):
            for to, cols in side_columns(jnp.where(k == 0, par_ref[0], 1 - par_ref[0]), buf.shape[2]):
                made[n, k, :, to] = buf[n, :, cols]
            done.append(pltpu.make_async_copy(made.at[n, k], out_ref.at[n, k], out_sem.at[2 * n + k]))
            done[-1].start()
    for copy in done:
        copy.wait()


def forward(mine_ref, low_ref, high_ref, own_ref, other_ref, out_ref, rows_ref, buf, sem, both, keep_sem, made, out_sem):
    jobs = [(w.at[n, k], buf.at[2 * p + n, k]) for p, w in enumerate((own_ref, other_ref)) for n in range(2) for k in range(2)]
    copies = [pltpu.make_async_copy(a, b, sem.at[i]) for i, (a, b) in enumerate(jobs)]
    for copy in copies:
        copy.start()
    rows = low_ref.shape[0]
    both[:rows] = low_ref[...]
    both[rows:] = high_ref[...]
    keep = [
        pltpu.make_async_copy(side, rows_ref.at[n], keep_sem.at[n])
        for n, side in enumerate((mine_ref, both))
    ]
    for copy in keep:
        copy.start()
    done = []

    def product(n):
        copies[2 * n].wait()
        copies[2 * n + 1].wait()
        return dot(mine_ref[...], buf[n, 0], NT) + dot(both[...], buf[n, 1], NT)

    for p in range(2):
        pre = product(2 * p)
        up = product(2 * p + 1)
        sig = jax.nn.sigmoid(pre)
        act = pre * sig
        made[p, 0] = (act * up).astype(BF16)
        made[p, 1] = (up * sig * (1.0 + pre * (1.0 - sig))).astype(BF16)
        made[p, 2] = act.astype(BF16)
        done.append(pltpu.make_async_copy(made.at[p], out_ref.at[p], out_sem.at[p]))
        done[-1].start()
    for copy in keep + done:
        copy.wait()


def hold(down_ref, out_ref, sem):
    copy = pltpu.make_async_copy(down_ref, out_ref, sem)
    copy.start()
    copy.wait()


def input_grad(grads, buf):
    total = dot(grads[0, 0], buf[0], NN)
    total += dot(grads[0, 1], buf[1], NN)
    total += dot(grads[1, 0], buf[2], NN)
    return total + dot(grads[1, 1], buf[3], NN)


def fetch_half(k, own_ref, other_ref, buf, sem):
    return [
        pltpu.make_async_copy(w.at[n, k], buf.at[2 * p + n], sem.at[2 * p + n])
        for p, w in enumerate((own_ref, other_ref))
        for n in range(2)
    ]


def backward(cot_ref, mid_ref, down0_ref, down1_ref, own_ref, other_ref, low_ref, high_ref, grads_ref, gate_ref, mid, mid_sem, wd, wd_sem, buf, sem, grads, out_sem):
    rows, width = cot_ref.shape
    mids = [pltpu.make_async_copy(mid_ref.at[p], mid.at[p], mid_sem.at[p]) for p in range(2)]
    second = pltpu.make_async_copy(down1_ref, wd, wd_sem)
    columns = fetch_half(1, own_ref, other_ref, buf, sem)
    for copy in (mids[0], second, mids[1], *columns):
        copy.start()
    gate = jnp.zeros((rows, 1), F32)
    done = []
    for p in range(2):
        if p == 1:
            second.wait()
        back = dot(cot_ref[...], (down0_ref, wd)[p][...], NT)
        mids[p].wait()
        gate = gate + jnp.sum(mid[p, 0].astype(F32) * back, axis=1, keepdims=True)
        grads[p, 0] = (back * mid[p, 1].astype(F32)).astype(BF16)
        grads[p, 1] = (back * mid[p, 2].astype(F32)).astype(BF16)
        done.append(pltpu.make_async_copy(grads.at[p], grads_ref.at[p], out_sem.at[p]))
        done[-1].start()
    wide = jnp.broadcast_to(gate, (rows, LANES))
    gate_ref[...] = wide
    low_ref[:, width // 2 :] = wide[: rows // 2].astype(BF16)
    high_ref[:, width // 2 :] = wide[rows // 2 :].astype(BF16)
    for copy in columns:
        copy.wait()
    total = input_grad(grads, buf).astype(BF16)
    low_ref[:, : width // 2] = total[: rows // 2]
    high_ref[:, : width // 2] = total[rows // 2 :]
    for copy in done:
        copy.wait()


def own_half(grads_ref, gate_ref, own_ref, other_ref, out_ref, grads, grad_sem, buf, sem):
    copies = [pltpu.make_async_copy(grads_ref.at[p], grads.at[p], grad_sem.at[p]) for p in range(2)]
    copies += fetch_half(0, own_ref, other_ref, buf, sem)
    for copy in copies:
        copy.start()
    part = buf.shape[2]
    out_ref[:, part:] = gate_ref[...]
    for copy in copies:
        copy.wait()
    out_ref[:, :part] = input_grad(grads, buf)


def add_pair(own_ref, low_ref, high_ref, out_ref, made, sem):
    rows = low_ref.shape[0]
    done = []
    for n, other in enumerate((low_ref, high_ref)):
        span = slice(n * rows, (n + 1) * rows)
        made[span] = (own_ref[span] + other[...].astype(F32)).astype(BF16)
        done.append(pltpu.make_async_copy(made.at[span], out_ref.at[span], sem.at[n]))
        done[-1].start()
    for copy in done:
        copy.wait()


def row_grads(p, par_ref, sides_ref, grads_ref, *refs):
    inputs = refs[:2] if p == 0 else ()
    outs, scratch = refs[len(inputs) : len(inputs) + 2], refs[len(inputs) + 2 :]
    sides, side_sem, left, left_sem, made, out_sem, *got = scratch
    keep = [pltpu.make_async_copy(sides_ref.at[k], sides.at[k], side_sem.at[k]) for k in range(2)]
    copies = [pltpu.make_async_copy(grads_ref.at[p, n], left.at[n], left_sem.at[n]) for n in range(2)]
    received = [pltpu.make_async_copy(r, got[0].at[n], got[1].at[n]) for n, r in enumerate(inputs)]
    for copy in (copies[0], *keep, copies[1], *received):
        copy.start()
    done = []
    for n in range(2):
        copies[n].wait()
        if p == 0:
            received[n].wait()
        for k, side in enumerate((par_ref[0], 1 - par_ref[0])):
            if n == 0:
                keep[k].wait()
            grad = dot(left[n], sides[k], TN)
            for to, cols in side_columns(side, made.shape[2]):
                piece = grad[:, to]
                if p == 0:
                    piece = piece + got[0][n, :, cols].astype(F32)
                made[n, :, cols] = piece.astype(BF16)
        done.append(pltpu.make_async_copy(made.at[n], outs[n], out_sem.at[n]))
        done[-1].start()
    for copy in done:
        copy.wait()


def down_grads(p, cot_ref, mid_ref, *refs):
    inputs, (out_ref, left, sem, made, out_sem, *got) = (refs[:1], refs[1:]) if p == 0 else ((), refs)
    copies = [pltpu.make_async_copy(mid_ref.at[p, 0], left, sem)]
    copies += [pltpu.make_async_copy(r, got[0], got[1]) for r in inputs]
    for copy in copies:
        copy.start()
    for copy in copies:
        copy.wait()
    grad = dot(left[...], cot_ref[...], TN)
    if p == 0:
        grad += got[0][...].astype(F32)
    made[...] = grad.astype(BF16)
    done = pltpu.make_async_copy(made, out_ref, out_sem)
    done.start()
    done.wait()


def combine(core_ref, table_ref, x_ref, keep_ref, send_ref):
    blocks, padded, _ = keep_ref.shape
    rows = table_ref.shape[1]
    width = 2 * blocks * LANES
    core = core_ref[0]
    masks = masks_of(table_slots(table_ref), x_ref.shape[0])
    grads = dot(pick_of(masks), x_ref[:, :width], TN)
    gate = x_ref[:, width : width + 1].astype(F32)
    lines = []
    for mask in masks:
        line = jnp.sum(jnp.where(mask, gate, 0.0), axis=0, keepdims=True)
        line = jnp.concatenate([line, jnp.zeros((1, 2 * LANES - rows), F32)], axis=1)
        lines += [line[:, :LANES], line[:, LANES:]]
    lines.append(jnp.zeros((padded - rows - len(lines), LANES), F32))
    tail = jnp.concatenate(lines, axis=0)
    for b in range(blocks):
        first = grads[:, 2 * b * LANES : (2 * b + 1) * LANES]
        second = grads[:, (2 * b + 1) * LANES : (2 * b + 2) * LANES]
        keep_ref[b, :rows, :] = jnp.where(core == 0, first, second)
        send_ref[b, :rows, :] = jnp.where(core == 0, second, first).astype(BF16)
        keep_ref[b, rows:, :] = tail
        send_ref[b, rows:, :] = tail.astype(BF16)


def join(turn_ref, keep_ref, got_ref, *out_refs):
    for k, out_ref in enumerate(out_refs):
        block = lax.rem(turn_ref[0] + k, len(out_refs))
        out_ref[...] = (keep_ref[block] + got_ref[block].astype(F32)).astype(BF16)


def finish(table_ref, *refs):
    parts, (tok_ref, gate_ref) = refs[:-2], refs[-2:]
    top_k, rows = gate_ref.shape
    total = functools.reduce(jnp.add, [x[...].astype(F32) for x in parts])
    tok_ref[...] = total[:rows].astype(BF16)
    for k in range(top_k):
        line = jnp.concatenate(
            [total[rows + 2 * k : rows + 2 * k + 1], total[rows + 2 * k + 1 : rows + 2 * k + 2]],
            axis=1,
        )
        gate_ref[k : k + 1, :] = line[:, :rows] / table_ref[top_k + k : top_k + k + 1, :]


def local(experts, tokens, cotangent, routing, gate_weights, gate_proj, up_proj, down_proj):
    rows, width = tokens.shape
    top_k = routing.shape[1]
    half = rows * top_k // experts
    count = experts * half
    part = width // 2
    depth = lax.axis_size(Z)
    core = lax.axis_index("c").astype(jnp.int32).reshape(1)
    parity = (lax.axis_index(Z) % 2).astype(jnp.int32).reshape(1)
    routes, gates = routing.T, gate_weights.T

    def swap(v):
        return lax.ppermute(v, "c", [(0, 1), (1, 0)])

    def shift(v, k):
        return lax.ppermute(v, Z, [(i, (i + k) % depth) for i in range(depth)])

    def exchange(v):
        return lax.all_to_all(v, EP, split_axis=0, concat_axis=0, tiled=True)

    dma = lambda n: pltpu.SemaphoreType.DMA((n,))

    ff = gate_proj.shape[2]
    down = down_proj[0]
    down_other = swap(down)
    (own,) = call(
        pack, [((2, 2, ff, part), BF16, "h")],
        (parity, "s"), (gate_proj[0].T, "h"), (up_proj[0].T, "h"),
        scratch=[
            pltpu.VMEM((2, ff, width), BF16), dma(2), pltpu.VMEM((2, 2, ff, part), BF16), dma(4),
        ],
        mib=10,
    )
    other = swap(own)
    (table,) = call(
        functools.partial(keep_table, experts, half), [((8, rows), F32, "v")],
        (core, "s"), (routes, "w"), (gates, "w"), mib=4,
    )

    (tok_out,) = call(
        functools.partial(send_tokens, experts, half),
        [((count, part), BF16, "h")],
        (core, "s"), (parity, "s"), (routes, "h"), (tokens, "h"),
        scratch=[
            pltpu.VMEM((top_k, rows), jnp.int32), pltpu.SemaphoreType.DMA,
            pltpu.VMEM((rows, part), BF16), dma(4), pltpu.VMEM((count, part), BF16), dma(2),
        ],
        flops=2 * count * rows * part, mib=8,
    )
    mine = exchange(tok_out.reshape(experts, half, part)).reshape(count, part)
    (cot_out,) = call(
        send_cotangents, [((count, width), BF16, "w")],
        (table, "v"), (cotangent, "w"),
        flops=2 * count * rows * width, mib=8,
    )
    cot = exchange(cot_out.reshape(experts, half, width)).reshape(count, width)
    low = shift(mine[: count // 2], 1)
    high = shift(mine[count // 2 :], -1)

    packed = [(own, "h"), (other, "h")]
    mids = pltpu.VMEM((2, 3, count, ff), BF16)
    halves = [pltpu.VMEM((4, ff, part), BF16), dma(4)]
    mid, sides = call(
        forward, [((2, 3, count, ff), BF16, "h"), ((2, count, part), BF16, "h")],
        (mine, "v"), (low, "v"), (high, "v"), *packed,
        scratch=[
            pltpu.VMEM((4, 2, ff, part), BF16), dma(8), pltpu.VMEM((count, part), BF16),
            dma(2), mids, dma(2),
        ],
        flops=8 * count * width * ff, mib=18,
    )
    (held,) = call(
        hold, [((ff, width), BF16, "v")], (down, "h"),
        scratch=[pltpu.SemaphoreType.DMA], mib=4,
    )
    message = ((count // 2, part + LANES), BF16, "v")
    to_low, to_high, grads, gate = call(
        backward,
        [message, message, ((2, 2, count, ff), BF16, "h"), ((count, LANES), F32, "v")],
        (cot, "v"), (mid, "h"), (held, "v"), (down_other, "h"), *packed,
        scratch=[
            mids, dma(2), pltpu.VMEM((ff, width), BF16), pltpu.SemaphoreType.DMA, *halves,
            pltpu.VMEM((2, 2, count, ff), BF16), dma(2),
        ],
        flops=8 * count * width * ff, mib=20,
    )
    from_low, from_high = shift(to_low, -1), shift(to_high, 1)
    (kept,) = call(
        own_half, [((count, part + LANES), F32, "v")],
        (grads, "h"), (gate, "v"), *packed,
        scratch=[pltpu.VMEM((2, 2, count, ff), BF16), dma(2), *halves],
        flops=4 * count * width * ff, mib=14,
    )
    (pair,) = call(
        add_pair, [((count, part + LANES), BF16, "h")], (kept, "v"), (from_low, "v"), (from_high, "v"),
        scratch=[pltpu.VMEM((count, part + LANES), BF16), dma(2)], mib=8,
    )
    returned = exchange(pair.reshape(experts, half, part + LANES)).reshape(count, part + LANES)

    one = pltpu.SemaphoreType.DMA
    shard = ((ff, width), BF16, "h")
    pair_room = pltpu.VMEM((2, ff, width), BF16)
    row_args = [(parity, "s"), (sides, "h"), (grads, "h")]
    row_room = [
        pltpu.VMEM((2, count, part), BF16), dma(2), pltpu.VMEM((2, count, ff), BF16), dma(2), pair_room, dma(2),
    ]
    down_args = [(cot, "v"), (mid, "h")]
    down_room = [pltpu.VMEM((count, ff), BF16), one, pltpu.VMEM((ff, width), BF16), one]
    cost = 2 * count * width * ff
    (their_down,) = call(
        functools.partial(down_grads, 1), [shard], *down_args,
        scratch=down_room, flops=cost, mib=10,
    )
    theirs = call(
        functools.partial(row_grads, 1), [shard] * 2, *row_args,
        scratch=row_room, flops=2 * cost, mib=14,
    )
    (grad_down,) = call(
        functools.partial(down_grads, 0), [shard], *down_args, (swap(their_down), "h"),
        scratch=[*down_room, down_room[2], one], flops=cost, mib=12,
    )
    received = [(swap(g), "h") for g in theirs]
    grad_gate, grad_up = call(
        functools.partial(row_grads, 0), [shard] * 2, *row_args, *received,
        scratch=[*row_room, pair_room, dma(2)], flops=2 * cost, mib=18,
    )

    block = (depth // 2, rows + 16, LANES)
    keep, send = call(
        combine, [(block, F32, "v"), (block, BF16, "v")],
        (core, "s"), (table, "v"), (returned, "v"),
        flops=2 * count * rows * part, mib=10,
    )
    turn = lax.axis_index("zh").astype(jnp.int32).reshape(1)
    steps = depth // 2
    parts = call(
        join, [(block[1:], BF16, "v")] * steps,
        (turn, "s"), (keep, "v"), (swap(send), "v"), mib=4,
    )
    sums = [parts[0]] + [shift(parts[k], 2 * k) for k in range(1, steps)]
    grad_tokens, grad_gates = call(
        finish,
        [((rows, LANES), BF16, "w"), ((top_k, rows), F32, "w")],
        (table, "v"), *((v, "v") for v in sums), mib=4,
    )
    return (grad_tokens, grad_gates.T, grad_gate.T[None], grad_up.T[None], grad_down[None])


def solution(mesh):
    devices = mesh.devices.reshape(4, 4, 4, 2, 2)
    inner = jax.sharding.Mesh(devices, (*EP, *Z, "c"))
    ep, tp = EP, (*Z, "c")

    def body(*args):
        return local(16, *args)

    return jax.shard_map(
        body,
        mesh=inner,
        in_specs=(
            P(ep, None),
            P(ep, None),
            P(ep, None),
            P(ep, None),
            P(ep, None, tp),
            P(ep, None, tp),
            P(ep, tp, None),
        ),
        out_specs=(
            P(ep, tp),
            P(ep, None),
            P(ep, None, tp),
            P(ep, None, tp),
            P(ep, tp, None),
        ),
        check_vma=False,
    )
```

```python
import functools

import jax
import jax.numpy as jnp
from jax import lax
from jax.experimental import pallas as pl
from jax.experimental.pallas import tpu as pltpu
from jax.sharding import PartitionSpec as P


EP = ("y", "x")
Z = ("zh", "zl")
LANES = 128
BF16 = jnp.bfloat16
F32 = jnp.float32
NN = (((1,), (0,)), ((), ()))
NT = (((1,), (1,)), ((), ()))
TN = (((0,), (0,)), ((), ()))
IN_VMEM = pl.BlockSpec(memory_space=pltpu.VMEM)
IN_HBM = pl.BlockSpec(memory_space=pltpu.HBM)
IN_SMEM = pl.BlockSpec(memory_space=pltpu.SMEM)


def dot(a, b, dims):
    return lax.dot_general(a, b, dims, preferred_element_type=F32)


def call(kernel, outs, *args, scratch=(), flops=0, mib=24):
    place = {"v": pltpu.VMEM, "h": pltpu.HBM, "w": pltpu.HBM}
    spec = {"v": IN_VMEM, "w": IN_VMEM, "h": IN_HBM, "s": IN_SMEM}
    moved = sum(a.size * a.dtype.itemsize for a, _ in args)
    kernel_call = pl.pallas_call(
        kernel,
        out_shape=[place[m](shape, dtype) for shape, dtype, m in outs],
        in_specs=[spec[m] for _, m in args],
        out_specs=[spec[m] for _, _, m in outs],
        scratch_shapes=list(scratch),
        cost_estimate=pl.CostEstimate(flops=flops, bytes_accessed=moved, transcendentals=0),
        compiler_params=pltpu.CompilerParams(vmem_limit_bytes=mib * 1024 * 1024),
    )
    return kernel_call(
        *(a if m == "s" else pltpu.with_memory_space_constraint(a, place[m]) for a, m in args)
    )


def slots_of(core, routes, experts, half):
    top_k, rows = routes.shape
    expert = lax.broadcasted_iota(jnp.int32, (experts, rows), 0)
    hits = [routes[k : k + 1, :] == expert for k in range(top_k)]
    named = functools.reduce(jnp.logical_or, hits)
    before = lax.broadcasted_iota(jnp.int32, (rows, rows), 0) < lax.broadcasted_iota(
        jnp.int32, (rows, rows), 1
    )
    ones = lambda mask: jnp.where(mask, 1.0, 0.0).astype(BF16)
    count = dot(ones(named), ones(before), NN)
    slots = []
    for k in range(top_k):
        place = jnp.sum(jnp.where(hits[k], count, 0.0), axis=0, keepdims=True).astype(jnp.int32)
        place = place - core * half
        inside = (place >= 0) & (place < half)
        slots.append(jnp.where(inside, routes[k : k + 1, :] * half + place, -1))
    return slots


def masks_of(slots, count):
    row = lax.broadcasted_iota(jnp.int32, (count, slots[0].shape[1]), 0)
    return [row == s for s in slots]


def pick_of(masks):
    hit = functools.reduce(jnp.logical_or, masks)
    return jnp.where(hit, 1.0, 0.0).astype(BF16)


def send_tokens(experts, half, core_ref, par_ref, routes_ref, tok_ref, out_ref, routes, route_sem, tok, sem, made, out_sem):
    route = pltpu.make_async_copy(routes_ref, routes, route_sem)
    route.start()
    copies = [
        pltpu.make_async_copy(tok_ref.at[:, cols], tok.at[:, to], sem.at[n])
        for n, (to, cols) in enumerate(side_columns(par_ref[0], tok_ref.shape[1]))
    ]
    for copy in copies:
        copy.start()
    route.wait()
    masks = masks_of(slots_of(core_ref[0], routes[...], experts, half), experts * half)
    for copy in copies:
        copy.wait()
    pick = pick_of(masks)
    part = out_ref.shape[1]
    done = []
    for n in range(2):
        cols = slice(n * part // 2, (n + 1) * part // 2)
        made[:, cols] = dot(pick, tok[:, cols], NN).astype(BF16)
        done.append(pltpu.make_async_copy(made.at[:, cols], out_ref.at[:, cols], out_sem.at[n]))
        done[-1].start()
    for copy in done:
        copy.wait()


def keep_table(experts, half, core_ref, routes_ref, gates_ref, out_ref):
    slots = slots_of(core_ref[0], routes_ref[...], experts, half)
    top_k = len(slots)
    gates = gates_ref[...].astype(F32)
    out_ref[...] = jnp.zeros(out_ref.shape, F32)
    for k in range(top_k):
        out_ref[k : k + 1] = slots[k].astype(F32)
        out_ref[top_k + k : top_k + k + 1] = gates[k : k + 1]


def table_slots(table_ref):
    return [table_ref[k : k + 1].astype(jnp.int32) for k in range(2)]


def send_cotangents(table_ref, cot_ref, out_ref):
    masks = masks_of(table_slots(table_ref), out_ref.shape[0])
    weigh = jnp.zeros(masks[0].shape, F32)
    for k, mask in enumerate(masks):
        weigh = jnp.where(mask, table_ref[2 + k : 3 + k], weigh)
    out_ref[...] = dot(weigh.astype(BF16), cot_ref[...], NN).astype(BF16)


def side_columns(side, width):
    step = width // 8
    return [
        (slice(m * step, (m + 1) * step), pl.ds(pl.multiple_of((2 * m + side) * step, step), step))
        for m in range(4)
    ]


def pack(par_ref, gate_ref, up_ref, out_ref, buf, sem, made, out_sem):
    copies = [pltpu.make_async_copy(w, buf.at[n], sem.at[n]) for n, w in enumerate((gate_ref, up_ref))]
    for copy in copies:
        copy.start()
    done = []
    for n, copy in enumerate(copies):
        copy.wait()
        for k in range(2):
            for to, cols in side_columns(jnp.where(k == 0, par_ref[0], 1 - par_ref[0]), buf.shape[2]):
                made[n, k, :, to] = buf[n, :, cols]
            done.append(pltpu.make_async_copy(made.at[n, k], out_ref.at[n, k], out_sem.at[2 * n + k]))
            done[-1].start()
    for copy in done:
        copy.wait()


def forward(mine_ref, low_ref, high_ref, own_ref, other_ref, out_ref, rows_ref, buf, sem, both, keep_sem, made, out_sem):
    jobs = [(w.at[n, k], buf.at[2 * p + n, k]) for p, w in enumerate((own_ref, other_ref)) for n in range(2) for k in range(2)]
    copies = [pltpu.make_async_copy(a, b, sem.at[i]) for i, (a, b) in enumerate(jobs)]
    for copy in copies:
        copy.start()
    rows = low_ref.shape[0]
    both[:rows] = low_ref[...]
    both[rows:] = high_ref[...]
    keep = [
        pltpu.make_async_copy(side, rows_ref.at[n], keep_sem.at[n])
        for n, side in enumerate((mine_ref, both))
    ]
    for copy in keep:
        copy.start()
    done = []

    def product(n):
        copies[2 * n].wait()
        copies[2 * n + 1].wait()
        return dot(mine_ref[...], buf[n, 0], NT) + dot(both[...], buf[n, 1], NT)

    for p in range(2):
        pre = product(2 * p)
        up = product(2 * p + 1)
        sig = jax.nn.sigmoid(pre)
        act = pre * sig
        made[p, 0] = (act * up).astype(BF16)
        made[p, 1] = (up * sig * (1.0 + pre * (1.0 - sig))).astype(BF16)
        made[p, 2] = act.astype(BF16)
        done.append(pltpu.make_async_copy(made.at[p], out_ref.at[p], out_sem.at[p]))
        done[-1].start()
    for copy in keep + done:
        copy.wait()


def hold(down_ref, out_ref, sem):
    copy = pltpu.make_async_copy(down_ref, out_ref, sem)
    copy.start()
    copy.wait()


def input_grad(grads, buf):
    total = dot(grads[0, 0], buf[0], NN)
    total += dot(grads[0, 1], buf[1], NN)
    total += dot(grads[1, 0], buf[2], NN)
    return total + dot(grads[1, 1], buf[3], NN)


def fetch_half(k, own_ref, other_ref, buf, sem):
    return [
        pltpu.make_async_copy(w.at[n, k], buf.at[2 * p + n], sem.at[2 * p + n])
        for p, w in enumerate((own_ref, other_ref))
        for n in range(2)
    ]


def backward(cot_ref, mid_ref, down0_ref, down1_ref, own_ref, other_ref, low_ref, high_ref, grads_ref, gate_ref, mid, mid_sem, wd, wd_sem, buf, sem, grads, out_sem):
    rows, width = cot_ref.shape
    mids = [pltpu.make_async_copy(mid_ref.at[p], mid.at[p], mid_sem.at[p]) for p in range(2)]
    second = pltpu.make_async_copy(down1_ref, wd, wd_sem)
    columns = fetch_half(1, own_ref, other_ref, buf, sem)
    for copy in (mids[0], second, mids[1], *columns):
        copy.start()
    gate = jnp.zeros((rows, 1), F32)
    done = []
    for p in range(2):
        if p == 1:
            second.wait()
        back = dot(cot_ref[...], (down0_ref, wd)[p][...], NT)
        mids[p].wait()
        gate = gate + jnp.sum(mid[p, 0].astype(F32) * back, axis=1, keepdims=True)
        grads[p, 0] = (back * mid[p, 1].astype(F32)).astype(BF16)
        grads[p, 1] = (back * mid[p, 2].astype(F32)).astype(BF16)
        done.append(pltpu.make_async_copy(grads.at[p], grads_ref.at[p], out_sem.at[p]))
        done[-1].start()
    wide = jnp.broadcast_to(gate, (rows, LANES))
    gate_ref[...] = wide
    low_ref[:, width // 2 :] = wide[: rows // 2].astype(BF16)
    high_ref[:, width // 2 :] = wide[rows // 2 :].astype(BF16)
    for copy in columns:
        copy.wait()
    total = input_grad(grads, buf).astype(BF16)
    low_ref[:, : width // 2] = total[: rows // 2]
    high_ref[:, : width // 2] = total[rows // 2 :]
    for copy in done:
        copy.wait()


def own_half(grads_ref, gate_ref, own_ref, other_ref, out_ref, grads, grad_sem, buf, sem):
    copies = [pltpu.make_async_copy(grads_ref.at[p], grads.at[p], grad_sem.at[p]) for p in range(2)]
    copies += fetch_half(0, own_ref, other_ref, buf, sem)
    for copy in copies:
        copy.start()
    part = buf.shape[2]
    out_ref[:, part:] = gate_ref[...]
    for copy in copies:
        copy.wait()
    out_ref[:, :part] = input_grad(grads, buf)


def add_pair(own_ref, low_ref, high_ref, out_ref, made, sem):
    rows = low_ref.shape[0]
    done = []
    for n, other in enumerate((low_ref, high_ref)):
        span = slice(n * rows, (n + 1) * rows)
        made[span] = (own_ref[span] + other[...].astype(F32)).astype(BF16)
        done.append(pltpu.make_async_copy(made.at[span], out_ref.at[span], sem.at[n]))
        done[-1].start()
    for copy in done:
        copy.wait()


def start_all(copies):
    for copy in copies:
        copy.start()
    return copies


def start_rows(p, sides_ref, grads_ref, inputs, scratch):
    sides, side_sem, left, left_sem, _, _, *got = scratch
    keep = [pltpu.make_async_copy(sides_ref.at[k], sides.at[k], side_sem.at[k]) for k in range(2)]
    copies = [pltpu.make_async_copy(grads_ref.at[p, n], left.at[n], left_sem.at[n]) for n in range(2)]
    received = [pltpu.make_async_copy(r, got[0].at[n], got[1].at[n]) for n, r in enumerate(inputs)]
    start_all([copies[0], *keep, copies[1], *received])
    return keep, copies, received


def finish_rows(par_ref, started, outs, scratch):
    keep, copies, received = started
    sides, _, left, _, made, out_sem, *got = scratch
    done = []
    for n in range(2):
        copies[n].wait()
        if received:
            received[n].wait()
        for k, side in enumerate((par_ref[0], 1 - par_ref[0])):
            if n == 0:
                keep[k].wait()
            grad = dot(left[n], sides[k], TN)
            for to, cols in side_columns(side, made.shape[2]):
                piece = grad[:, to]
                if received:
                    piece = piece + got[0][n, :, cols].astype(F32)
                made[n, :, cols] = piece.astype(BF16)
        done += start_all([pltpu.make_async_copy(made.at[n], outs[n], out_sem.at[n])])
    return done


def start_down(p, mid_ref, inputs, scratch):
    left, sem, _, _, *got = scratch
    copies = [pltpu.make_async_copy(mid_ref.at[p, 0], left, sem)]
    return start_all(copies + [pltpu.make_async_copy(r, got[0], got[1]) for r in inputs])


def finish_down(cot_ref, started, out_ref, scratch):
    left, _, made, out_sem, *got = scratch
    for copy in started:
        copy.wait()
    grad = dot(left[...], cot_ref[...], TN)
    if got:
        grad += got[0][...].astype(F32)
    made[...] = grad.astype(BF16)
    return start_all([pltpu.make_async_copy(made, out_ref, out_sem)])


def their_down_grads(cot_ref, mid_ref, out_ref, *scratch):
    for copy in finish_down(cot_ref, start_down(1, mid_ref, (), scratch), out_ref, scratch):
        copy.wait()


def middle_grads(par_ref, sides_ref, grads_ref, cot_ref, mid_ref, got_ref, gate_ref, up_ref, down_ref, *scratch):
    rows, down = scratch[:6], scratch[6:]
    started = start_rows(1, sides_ref, grads_ref, (), rows)
    down_started = start_down(0, mid_ref, (got_ref,), down)
    done = finish_rows(par_ref, started, (gate_ref, up_ref), rows)
    done += finish_down(cot_ref, down_started, down_ref, down)
    for copy in done:
        copy.wait()


def own_row_grads(par_ref, sides_ref, grads_ref, got0_ref, got1_ref, gate_ref, up_ref, *scratch):
    started = start_rows(0, sides_ref, grads_ref, (got0_ref, got1_ref), scratch)
    for copy in finish_rows(par_ref, started, (gate_ref, up_ref), scratch):
        copy.wait()


def combine(core_ref, table_ref, x_ref, keep_ref, send_ref):
    blocks, padded, _ = keep_ref.shape
    rows = table_ref.shape[1]
    width = 2 * blocks * LANES
    core = core_ref[0]
    masks = masks_of(table_slots(table_ref), x_ref.shape[0])
    grads = dot(pick_of(masks), x_ref[:, :width], TN)
    gate = x_ref[:, width : width + 1].astype(F32)
    lines = []
    for mask in masks:
        line = jnp.sum(jnp.where(mask, gate, 0.0), axis=0, keepdims=True)
        line = jnp.concatenate([line, jnp.zeros((1, 2 * LANES - rows), F32)], axis=1)
        lines += [line[:, :LANES], line[:, LANES:]]
    lines.append(jnp.zeros((padded - rows - len(lines), LANES), F32))
    tail = jnp.concatenate(lines, axis=0)
    for b in range(blocks):
        first = grads[:, 2 * b * LANES : (2 * b + 1) * LANES]
        second = grads[:, (2 * b + 1) * LANES : (2 * b + 2) * LANES]
        keep_ref[b, :rows, :] = jnp.where(core == 0, first, second)
        send_ref[b, :rows, :] = jnp.where(core == 0, second, first).astype(BF16)
        keep_ref[b, rows:, :] = tail
        send_ref[b, rows:, :] = tail.astype(BF16)


def join(turn_ref, keep_ref, got_ref, *out_refs):
    for k, out_ref in enumerate(out_refs):
        block = lax.rem(turn_ref[0] + k, len(out_refs))
        out_ref[...] = (keep_ref[block] + got_ref[block].astype(F32)).astype(BF16)


def finish(table_ref, *refs):
    parts, (tok_ref, gate_ref) = refs[:-2], refs[-2:]
    top_k, rows = gate_ref.shape
    total = functools.reduce(jnp.add, [x[...].astype(F32) for x in parts])
    tok_ref[...] = total[:rows].astype(BF16)
    for k in range(top_k):
        line = jnp.concatenate(
            [total[rows + 2 * k : rows + 2 * k + 1], total[rows + 2 * k + 1 : rows + 2 * k + 2]],
            axis=1,
        )
        gate_ref[k : k + 1, :] = line[:, :rows] / table_ref[top_k + k : top_k + k + 1, :]


def local(experts, tokens, cotangent, routing, gate_weights, gate_proj, up_proj, down_proj):
    rows, width = tokens.shape
    top_k = routing.shape[1]
    half = rows * top_k // experts
    count = experts * half
    part = width // 2
    depth = lax.axis_size(Z)
    core = lax.axis_index("c").astype(jnp.int32).reshape(1)
    parity = (lax.axis_index(Z) % 2).astype(jnp.int32).reshape(1)
    routes, gates = routing.T, gate_weights.T

    def swap(v):
        return lax.ppermute(v, "c", [(0, 1), (1, 0)])

    def shift(v, k):
        return lax.ppermute(v, Z, [(i, (i + k) % depth) for i in range(depth)])

    def exchange(v):
        return lax.all_to_all(v, EP, split_axis=0, concat_axis=0, tiled=True)

    dma = lambda n: pltpu.SemaphoreType.DMA((n,))

    ff = gate_proj.shape[2]
    down = down_proj[0]
    down_other = swap(down)
    (own,) = call(
        pack, [((2, 2, ff, part), BF16, "h")],
        (parity, "s"), (gate_proj[0].T, "h"), (up_proj[0].T, "h"),
        scratch=[
            pltpu.VMEM((2, ff, width), BF16), dma(2), pltpu.VMEM((2, 2, ff, part), BF16), dma(4),
        ],
        mib=10,
    )
    other = swap(own)
    (table,) = call(
        functools.partial(keep_table, experts, half), [((8, rows), F32, "v")],
        (core, "s"), (routes, "w"), (gates, "w"), mib=4,
    )

    (tok_out,) = call(
        functools.partial(send_tokens, experts, half),
        [((count, part), BF16, "h")],
        (core, "s"), (parity, "s"), (routes, "h"), (tokens, "h"),
        scratch=[
            pltpu.VMEM((top_k, rows), jnp.int32), pltpu.SemaphoreType.DMA,
            pltpu.VMEM((rows, part), BF16), dma(4), pltpu.VMEM((count, part), BF16), dma(2),
        ],
        flops=2 * count * rows * part, mib=8,
    )
    mine = exchange(tok_out.reshape(experts, half, part)).reshape(count, part)
    (cot_out,) = call(
        send_cotangents, [((count, width), BF16, "w")],
        (table, "v"), (cotangent, "w"),
        flops=2 * count * rows * width, mib=8,
    )
    cot = exchange(cot_out.reshape(experts, half, width)).reshape(count, width)
    low = shift(mine[: count // 2], 1)
    high = shift(mine[count // 2 :], -1)

    packed = [(own, "h"), (other, "h")]
    mids = pltpu.VMEM((2, 3, count, ff), BF16)
    halves = [pltpu.VMEM((4, ff, part), BF16), dma(4)]
    mid, sides = call(
        forward, [((2, 3, count, ff), BF16, "h"), ((2, count, part), BF16, "h")],
        (mine, "v"), (low, "v"), (high, "v"), *packed,
        scratch=[
            pltpu.VMEM((4, 2, ff, part), BF16), dma(8), pltpu.VMEM((count, part), BF16),
            dma(2), mids, dma(2),
        ],
        flops=8 * count * width * ff, mib=18,
    )
    (held,) = call(
        hold, [((ff, width), BF16, "v")], (down, "h"),
        scratch=[pltpu.SemaphoreType.DMA], mib=4,
    )
    message = ((count // 2, part + LANES), BF16, "v")
    to_low, to_high, grads, gate = call(
        backward,
        [message, message, ((2, 2, count, ff), BF16, "h"), ((count, LANES), F32, "v")],
        (cot, "v"), (mid, "h"), (held, "v"), (down_other, "h"), *packed,
        scratch=[
            mids, dma(2), pltpu.VMEM((ff, width), BF16), pltpu.SemaphoreType.DMA, *halves,
            pltpu.VMEM((2, 2, count, ff), BF16), dma(2),
        ],
        flops=8 * count * width * ff, mib=20,
    )
    from_low, from_high = shift(to_low, -1), shift(to_high, 1)
    (kept,) = call(
        own_half, [((count, part + LANES), F32, "v")],
        (grads, "h"), (gate, "v"), *packed,
        scratch=[pltpu.VMEM((2, 2, count, ff), BF16), dma(2), *halves],
        flops=4 * count * width * ff, mib=14,
    )
    (pair,) = call(
        add_pair, [((count, part + LANES), BF16, "h")], (kept, "v"), (from_low, "v"), (from_high, "v"),
        scratch=[pltpu.VMEM((count, part + LANES), BF16), dma(2)], mib=8,
    )
    returned = exchange(pair.reshape(experts, half, part + LANES)).reshape(count, part + LANES)

    one = pltpu.SemaphoreType.DMA
    shard = ((ff, width), BF16, "h")
    pair_room = pltpu.VMEM((2, ff, width), BF16)
    row_args = [(parity, "s"), (sides, "h"), (grads, "h")]
    row_room = [
        pltpu.VMEM((2, count, part), BF16), dma(2), pltpu.VMEM((2, count, ff), BF16), dma(2), pair_room, dma(2),
    ]
    down_args = [(cot, "v"), (mid, "h")]
    down_room = [pltpu.VMEM((count, ff), BF16), one, pltpu.VMEM((ff, width), BF16), one]
    cost = 2 * count * width * ff
    (their_down,) = call(their_down_grads, [shard], *down_args, scratch=down_room, flops=cost, mib=10)
    *theirs, grad_down = call(
        middle_grads, [shard] * 3, *row_args, *down_args, (swap(their_down), "h"),
        scratch=[*row_room, *down_room, down_room[2], one], flops=3 * cost, mib=20,
    )
    received = [(swap(g), "h") for g in theirs]
    grad_gate, grad_up = call(
        own_row_grads, [shard] * 2, *row_args, *received,
        scratch=[*row_room, pair_room, dma(2)], flops=2 * cost, mib=18,
    )

    block = (depth // 2, rows + 16, LANES)
    keep, send = call(
        combine, [(block, F32, "v"), (block, BF16, "v")],
        (core, "s"), (table, "v"), (returned, "v"),
        flops=2 * count * rows * part, mib=10,
    )
    turn = lax.axis_index("zh").astype(jnp.int32).reshape(1)
    steps = depth // 2
    parts = call(
        join, [(block[1:], BF16, "v")] * steps,
        (turn, "s"), (keep, "v"), (swap(send), "v"), mib=4,
    )
    sums = [parts[0]] + [shift(parts[k], 2 * k) for k in range(1, steps)]
    grad_tokens, grad_gates = call(
        finish,
        [((rows, LANES), BF16, "w"), ((top_k, rows), F32, "w")],
        (table, "v"), *((v, "v") for v in sums), mib=4,
    )
    return (grad_tokens, grad_gates.T, grad_gate.T[None], grad_up.T[None], grad_down[None])


def solution(mesh):
    devices = mesh.devices.reshape(4, 4, 4, 2, 2)
    inner = jax.sharding.Mesh(devices, (*EP, *Z, "c"))
    ep, tp = EP, (*Z, "c")

    def body(*args):
        return local(16, *args)

    return jax.shard_map(
        body,
        mesh=inner,
        in_specs=(
            P(ep, None),
            P(ep, None),
            P(ep, None),
            P(ep, None),
            P(ep, None, tp),
            P(ep, None, tp),
            P(ep, tp, None),
        ),
        out_specs=(
            P(ep, tp),
            P(ep, None),
            P(ep, None, tp),
            P(ep, None, tp),
            P(ep, tp, None),
        ),
        check_vma=False,
    )
```

```python
import functools

import jax
import jax.numpy as jnp
from jax import lax
from jax.experimental import pallas as pl
from jax.experimental.pallas import tpu as pltpu
from jax.sharding import PartitionSpec as P


EP = ("y", "x")
Z = ("zh", "zl")
LANES = 128
BF16 = jnp.bfloat16
F32 = jnp.float32
NN = (((1,), (0,)), ((), ()))
NT = (((1,), (1,)), ((), ()))
TN = (((0,), (0,)), ((), ()))
IN_VMEM = pl.BlockSpec(memory_space=pltpu.VMEM)
IN_HBM = pl.BlockSpec(memory_space=pltpu.HBM)
IN_SMEM = pl.BlockSpec(memory_space=pltpu.SMEM)


def dot(a, b, dims):
    return lax.dot_general(a, b, dims, preferred_element_type=F32)


def call(kernel, outs, *args, scratch=(), flops=0, mib=24):
    place = {"v": pltpu.VMEM, "h": pltpu.HBM, "w": pltpu.HBM}
    spec = {"v": IN_VMEM, "w": IN_VMEM, "h": IN_HBM, "s": IN_SMEM}
    moved = sum(a.size * a.dtype.itemsize for a, _ in args)
    kernel_call = pl.pallas_call(
        kernel,
        out_shape=[place[m](shape, dtype) for shape, dtype, m in outs],
        in_specs=[spec[m] for _, m in args],
        out_specs=[spec[m] for _, _, m in outs],
        scratch_shapes=list(scratch),
        cost_estimate=pl.CostEstimate(flops=flops, bytes_accessed=moved, transcendentals=0),
        compiler_params=pltpu.CompilerParams(vmem_limit_bytes=mib * 1024 * 1024),
    )
    return kernel_call(
        *(a if m == "s" else pltpu.with_memory_space_constraint(a, place[m]) for a, m in args)
    )


def slots_of(core, routes, experts, half):
    top_k, rows = routes.shape
    expert = lax.broadcasted_iota(jnp.int32, (experts, rows), 0)
    hits = [routes[k : k + 1, :] == expert for k in range(top_k)]
    named = functools.reduce(jnp.logical_or, hits)
    before = lax.broadcasted_iota(jnp.int32, (rows, rows), 0) < lax.broadcasted_iota(
        jnp.int32, (rows, rows), 1
    )
    ones = lambda mask: jnp.where(mask, 1.0, 0.0).astype(BF16)
    count = dot(ones(named), ones(before), NN)
    slots = []
    for k in range(top_k):
        place = jnp.sum(jnp.where(hits[k], count, 0.0), axis=0, keepdims=True).astype(jnp.int32)
        place = place - core * half
        inside = (place >= 0) & (place < half)
        slots.append(jnp.where(inside, routes[k : k + 1, :] * half + place, -1))
    return slots


def masks_of(slots, count):
    row = lax.broadcasted_iota(jnp.int32, (count, slots[0].shape[1]), 0)
    return [row == s for s in slots]


def pick_of(masks):
    hit = functools.reduce(jnp.logical_or, masks)
    return jnp.where(hit, 1.0, 0.0).astype(BF16)


def send_tokens(experts, half, core_ref, par_ref, routes_ref, tok_ref, out_ref, routes, route_sem, tok, sem, made, out_sem):
    route = pltpu.make_async_copy(routes_ref, routes, route_sem)
    route.start()
    copies = [
        pltpu.make_async_copy(tok_ref.at[:, cols], tok.at[:, to], sem.at[n])
        for n, (to, cols) in enumerate(side_columns(par_ref[0], tok_ref.shape[1]))
    ]
    for copy in copies:
        copy.start()
    route.wait()
    masks = masks_of(slots_of(core_ref[0], routes[...], experts, half), experts * half)
    for copy in copies:
        copy.wait()
    pick = pick_of(masks)
    part = out_ref.shape[1]
    done = []
    for n in range(2):
        cols = slice(n * part // 2, (n + 1) * part // 2)
        made[:, cols] = dot(pick, tok[:, cols], NN).astype(BF16)
        done.append(pltpu.make_async_copy(made.at[:, cols], out_ref.at[:, cols], out_sem.at[n]))
        done[-1].start()
    for copy in done:
        copy.wait()


def keep_table(experts, half, core_ref, routes_ref, gates_ref, out_ref):
    slots = slots_of(core_ref[0], routes_ref[...], experts, half)
    top_k = len(slots)
    gates = gates_ref[...].astype(F32)
    out_ref[...] = jnp.zeros(out_ref.shape, F32)
    for k in range(top_k):
        out_ref[k : k + 1] = slots[k].astype(F32)
        out_ref[top_k + k : top_k + k + 1] = gates[k : k + 1]


def table_slots(table_ref):
    return [table_ref[k : k + 1].astype(jnp.int32) for k in range(2)]


def send_cotangents(table_ref, cot_ref, out_ref):
    masks = masks_of(table_slots(table_ref), out_ref.shape[0])
    weigh = jnp.zeros(masks[0].shape, F32)
    for k, mask in enumerate(masks):
        weigh = jnp.where(mask, table_ref[2 + k : 3 + k], weigh)
    out_ref[...] = dot(weigh.astype(BF16), cot_ref[...], NN).astype(BF16)


def side_columns(side, width):
    step = width // 8
    return [
        (slice(m * step, (m + 1) * step), pl.ds(pl.multiple_of((2 * m + side) * step, step), step))
        for m in range(4)
    ]


def pack(par_ref, gate_ref, up_ref, out_ref, buf, sem, made, out_sem):
    copies = [pltpu.make_async_copy(w, buf.at[n], sem.at[n]) for n, w in enumerate((gate_ref, up_ref))]
    for copy in copies:
        copy.start()
    done = []
    for n, copy in enumerate(copies):
        copy.wait()
        for k in range(2):
            for to, cols in side_columns(jnp.where(k == 0, par_ref[0], 1 - par_ref[0]), buf.shape[2]):
                made[n, k, :, to] = buf[n, :, cols]
            done.append(pltpu.make_async_copy(made.at[n, k], out_ref.at[n, k], out_sem.at[2 * n + k]))
            done[-1].start()
    for copy in done:
        copy.wait()


def forward(mine_ref, low_ref, high_ref, own_ref, other_ref, out_ref, rows_ref, hid_ref, buf, sem, both, keep_sem, made, out_sem):
    jobs = [(w.at[n, k], buf.at[2 * p + n, k]) for p, w in enumerate((own_ref, other_ref)) for n in range(2) for k in range(2)]
    copies = [pltpu.make_async_copy(a, b, sem.at[i]) for i, (a, b) in enumerate(jobs)]
    for copy in copies:
        copy.start()
    rows = low_ref.shape[0]
    both[:rows] = low_ref[...]
    both[rows:] = high_ref[...]
    keep = [
        pltpu.make_async_copy(side, rows_ref.at[n], keep_sem.at[n])
        for n, side in enumerate((mine_ref, both))
    ]
    for copy in keep:
        copy.start()
    done = []

    def product(n):
        copies[2 * n].wait()
        copies[2 * n + 1].wait()
        return dot(mine_ref[...], buf[n, 0], NT) + dot(both[...], buf[n, 1], NT)

    for p in range(2):
        pre = product(2 * p)
        up = product(2 * p + 1)
        sig = jax.nn.sigmoid(pre)
        act = pre * sig
        made[p, 0] = (act * up).astype(BF16)
        made[p, 1] = (up * sig * (1.0 + pre * (1.0 - sig))).astype(BF16)
        made[p, 2] = act.astype(BF16)
        done.append(pltpu.make_async_copy(made.at[p], out_ref.at[p], out_sem.at[p]))
        done[-1].start()
    done.append(pltpu.make_async_copy(made.at[1, 0], hid_ref, out_sem.at[2]))
    done[-1].start()
    for copy in keep + done:
        copy.wait()


def hold(down_ref, out_ref, sem):
    copy = pltpu.make_async_copy(down_ref, out_ref, sem)
    copy.start()
    copy.wait()


def input_grad(grads, buf):
    total = dot(grads[0, 0], buf[0], NN)
    total += dot(grads[0, 1], buf[1], NN)
    total += dot(grads[1, 0], buf[2], NN)
    return total + dot(grads[1, 1], buf[3], NN)


def fetch_half(k, own_ref, other_ref, buf, sem):
    return [
        pltpu.make_async_copy(w.at[n, k], buf.at[2 * p + n], sem.at[2 * p + n])
        for p, w in enumerate((own_ref, other_ref))
        for n in range(2)
    ]


def backward(cot_ref, mid_ref, down0_ref, down1_ref, own_ref, other_ref, low_ref, high_ref, grads_ref, theirs_ref, gate_ref, mid, mid_sem, wd, wd_sem, buf, sem, grads, out_sem, wide_grads):
    rows, width = cot_ref.shape
    mids = [pltpu.make_async_copy(mid_ref.at[p], mid.at[p], mid_sem.at[p]) for p in range(2)]
    second = pltpu.make_async_copy(down1_ref, wd, wd_sem)
    columns = fetch_half(1, own_ref, other_ref, buf, sem)
    for copy in (mids[0], second, mids[1], *columns):
        copy.start()
    gate = jnp.zeros((rows, 1), F32)
    done = []
    for p in range(2):
        if p == 1:
            second.wait()
        back = dot(cot_ref[...], (down0_ref, wd)[p][...], NT)
        mids[p].wait()
        gate = gate + jnp.sum(mid[p, 0].astype(F32) * back, axis=1, keepdims=True)
        grads[p, 0] = (back * mid[p, 1].astype(F32)).astype(BF16)
        grads[p, 1] = (back * mid[p, 2].astype(F32)).astype(BF16)
        for n in range(2):
            if p == 0:
                source, to = grads.at[0, n], grads_ref.at[n]
            else:
                wide_grads[n] = jnp.zeros(wide_grads.shape[1:], BF16)
                wide_grads[n, :, : grads.shape[3]] = grads[1, n]
                source, to = wide_grads.at[n], theirs_ref.at[n * rows : (n + 1) * rows]
            done.append(pltpu.make_async_copy(source, to, out_sem.at[2 * p + n]))
            done[-1].start()
    wide = jnp.broadcast_to(gate, (rows, LANES))
    gate_ref[...] = wide
    low_ref[:, width // 2 :] = wide[: rows // 2].astype(BF16)
    high_ref[:, width // 2 :] = wide[rows // 2 :].astype(BF16)
    for copy in columns:
        copy.wait()
    total = input_grad(grads, buf).astype(BF16)
    low_ref[:, : width // 2] = total[: rows // 2]
    high_ref[:, : width // 2] = total[rows // 2 :]
    for copy in done:
        copy.wait()


def own_half(grads_ref, theirs_ref, gate_ref, own_ref, other_ref, out_ref, grads, grad_sem, buf, sem, wide):
    rows = gate_ref.shape[0]
    copies = [pltpu.make_async_copy(grads_ref, grads.at[0], grad_sem.at[2])]
    copies += [
        pltpu.make_async_copy(theirs_ref.at[n * rows : (n + 1) * rows], wide.at[n], grad_sem.at[n])
        for n in range(2)
    ]
    copies += fetch_half(0, own_ref, other_ref, buf, sem)
    for copy in copies:
        copy.start()
    part = buf.shape[2]
    out_ref[:, part:] = gate_ref[...]
    for copy in copies:
        copy.wait()
    for n in range(2):
        grads[1, n] = wide[n, :, : grads.shape[3]]
    out_ref[:, :part] = input_grad(grads, buf)


def add_pair(own_ref, low_ref, high_ref, out_ref, made, sem):
    rows = low_ref.shape[0]
    done = []
    for n, other in enumerate((low_ref, high_ref)):
        span = slice(n * rows, (n + 1) * rows)
        made[span] = (own_ref[span] + other[...].astype(F32)).astype(BF16)
        done.append(pltpu.make_async_copy(made.at[span], out_ref.at[span], sem.at[n]))
        done[-1].start()
    for copy in done:
        copy.wait()


def start_all(copies):
    for copy in copies:
        copy.start()
    return copies


def row_grads(par_ref, *refs):
    inputs, outs, (sides, side_sem, left, left_sem, made, out_sem, wide) = refs[:4], refs[4:6], refs[6:]
    rows, ff = left.shape[1:]
    sources = [
        [inputs[2].at[n] for n in range(2)],
        [inputs[3].at[n * rows : (n + 1) * rows] for n in range(2)],
    ]
    lefts = [
        [pltpu.make_async_copy(sources[q][n], (left, wide)[q].at[n], left_sem.at[2 * q + n]) for n in range(2)]
        for q in range(2)
    ]
    rights = [
        [pltpu.make_async_copy(inputs[q].at[k], sides.at[q, k], side_sem.at[2 * q + k]) for k in range(2)]
        for q in range(2)
    ]
    for q in range(2):
        start_all([lefts[q][0], *rights[q], lefts[q][1]])
    done = []
    for n in range(2):
        for k, side in enumerate((par_ref[0], 1 - par_ref[0])):
            total = 0.0
            for q in range(2):
                if k == 0:
                    lefts[q][n].wait()
                if n == 0:
                    rights[q][k].wait()
                side_left = left[n] if q == 0 else wide[n, :, :ff]
                total = total + dot(side_left, sides[q, k], TN)
            for to, cols in side_columns(side, made.shape[2]):
                made[n, :, cols] = total[:, to].astype(BF16)
        done += start_all([pltpu.make_async_copy(made.at[n], outs[n], out_sem.at[n])])
    for copy in done:
        copy.wait()


def down_grads(cot_ref, mid_ref, cot1_ref, hid1_ref, out_ref, left, left_sem, cot1, cot_sem, made, out_sem):
    copies = start_all([
        pltpu.make_async_copy(mid_ref.at[0, 0], left.at[0], left_sem.at[0]),
        pltpu.make_async_copy(cot1_ref, cot1, cot_sem),
        pltpu.make_async_copy(hid1_ref, left.at[1], left_sem.at[1]),
    ])
    copies[0].wait()
    total = dot(left[0], cot_ref[...], TN)
    copies[1].wait()
    copies[2].wait()
    made[...] = (total + dot(left[1], cot1[...], TN)).astype(BF16)
    done = pltpu.make_async_copy(made, out_ref, out_sem)
    done.start()
    done.wait()


def combine(core_ref, table_ref, x_ref, keep_ref, send_ref):
    blocks, padded, _ = keep_ref.shape
    rows = table_ref.shape[1]
    width = 2 * blocks * LANES
    core = core_ref[0]
    masks = masks_of(table_slots(table_ref), x_ref.shape[0])
    grads = dot(pick_of(masks), x_ref[:, :width], TN)
    gate = x_ref[:, width : width + 1].astype(F32)
    lines = []
    for mask in masks:
        line = jnp.sum(jnp.where(mask, gate, 0.0), axis=0, keepdims=True)
        line = jnp.concatenate([line, jnp.zeros((1, 2 * LANES - rows), F32)], axis=1)
        lines += [line[:, :LANES], line[:, LANES:]]
    lines.append(jnp.zeros((padded - rows - len(lines), LANES), F32))
    tail = jnp.concatenate(lines, axis=0)
    for b in range(blocks):
        first = grads[:, 2 * b * LANES : (2 * b + 1) * LANES]
        second = grads[:, (2 * b + 1) * LANES : (2 * b + 2) * LANES]
        keep_ref[b, :rows, :] = jnp.where(core == 0, first, second)
        send_ref[b, :rows, :] = jnp.where(core == 0, second, first).astype(BF16)
        keep_ref[b, rows:, :] = tail
        send_ref[b, rows:, :] = tail.astype(BF16)


def join(turn_ref, keep_ref, got_ref, *out_refs):
    for k, out_ref in enumerate(out_refs):
        block = lax.rem(turn_ref[0] + k, len(out_refs))
        out_ref[...] = (keep_ref[block] + got_ref[block].astype(F32)).astype(BF16)


def finish(table_ref, *refs):
    parts, (tok_ref, gate_ref) = refs[:-2], refs[-2:]
    top_k, rows = gate_ref.shape
    total = functools.reduce(jnp.add, [x[...].astype(F32) for x in parts])
    tok_ref[...] = total[:rows].astype(BF16)
    for k in range(top_k):
        line = jnp.concatenate(
            [total[rows + 2 * k : rows + 2 * k + 1], total[rows + 2 * k + 1 : rows + 2 * k + 2]],
            axis=1,
        )
        gate_ref[k : k + 1, :] = line[:, :rows] / table_ref[top_k + k : top_k + k + 1, :]


def local(experts, tokens, cotangent, routing, gate_weights, gate_proj, up_proj, down_proj):
    rows, width = tokens.shape
    top_k = routing.shape[1]
    half = rows * top_k // experts
    count = experts * half
    part = width // 2
    depth = lax.axis_size(Z)
    core = lax.axis_index("c").astype(jnp.int32).reshape(1)
    parity = (lax.axis_index(Z) % 2).astype(jnp.int32).reshape(1)
    routes, gates = routing.T, gate_weights.T

    def swap(v):
        return lax.ppermute(v, "c", [(0, 1), (1, 0)])

    def shift(v, k):
        return lax.ppermute(v, Z, [(i, (i + k) % depth) for i in range(depth)])

    def exchange(v):
        return lax.all_to_all(v, EP, split_axis=0, concat_axis=0, tiled=True)

    dma = lambda n: pltpu.SemaphoreType.DMA((n,))

    ff = gate_proj.shape[2]
    down = down_proj[0]
    down_other = swap(down)
    (own,) = call(
        pack, [((2, 2, ff, part), BF16, "h")],
        (parity, "s"), (gate_proj[0].T, "h"), (up_proj[0].T, "h"),
        scratch=[
            pltpu.VMEM((2, ff, width), BF16), dma(2), pltpu.VMEM((2, 2, ff, part), BF16), dma(4),
        ],
        mib=10,
    )
    other = swap(own)
    (table,) = call(
        functools.partial(keep_table, experts, half), [((8, rows), F32, "v")],
        (core, "s"), (routes, "w"), (gates, "w"), mib=4,
    )

    (tok_out,) = call(
        functools.partial(send_tokens, experts, half),
        [((count, part), BF16, "h")],
        (core, "s"), (parity, "s"), (routes, "h"), (tokens, "h"),
        scratch=[
            pltpu.VMEM((top_k, rows), jnp.int32), pltpu.SemaphoreType.DMA,
            pltpu.VMEM((rows, part), BF16), dma(4), pltpu.VMEM((count, part), BF16), dma(2),
        ],
        flops=2 * count * rows * part, mib=8,
    )
    mine = exchange(tok_out.reshape(experts, half, part)).reshape(count, part)
    (cot_out,) = call(
        send_cotangents, [((count, width), BF16, "w")],
        (table, "v"), (cotangent, "w"),
        flops=2 * count * rows * width, mib=8,
    )
    cot = exchange(cot_out.reshape(experts, half, width)).reshape(count, width)
    low = shift(mine[: count // 2], 1)
    high = shift(mine[count // 2 :], -1)

    packed = [(own, "h"), (other, "h")]
    mids = pltpu.VMEM((2, 3, count, ff), BF16)
    halves = [pltpu.VMEM((4, ff, part), BF16), dma(4)]
    mid, sides, hid = call(
        forward,
        [((2, 3, count, ff), BF16, "h"), ((2, count, part), BF16, "h"), ((count, ff), BF16, "h")],
        (mine, "v"), (low, "v"), (high, "v"), *packed,
        scratch=[
            pltpu.VMEM((4, 2, ff, part), BF16), dma(8), pltpu.VMEM((count, part), BF16),
            dma(2), mids, dma(3),
        ],
        flops=8 * count * width * ff, mib=18,
    )
    (held,) = call(
        hold, [((ff, width), BF16, "v")], (down, "h"),
        scratch=[pltpu.SemaphoreType.DMA], mib=4,
    )
    padded = (ff + LANES - 1) // LANES * LANES
    message = ((count // 2, part + LANES), BF16, "v")
    to_low, to_high, grads, theirs, gate = call(
        backward,
        [
            message, message, ((2, count, ff), BF16, "h"), ((2 * count, padded), BF16, "h"),
            ((count, LANES), F32, "v"),
        ],
        (cot, "v"), (mid, "h"), (held, "v"), (down_other, "h"), *packed,
        scratch=[
            mids, dma(2), pltpu.VMEM((ff, width), BF16), pltpu.SemaphoreType.DMA, *halves,
            pltpu.VMEM((2, 2, count, ff), BF16), dma(4), pltpu.VMEM((2, count, padded), BF16),
        ],
        flops=8 * count * width * ff, mib=20,
    )
    from_low, from_high = shift(to_low, -1), shift(to_high, 1)
    (kept,) = call(
        own_half, [((count, part + LANES), F32, "v")],
        (grads, "h"), (theirs, "h"), (gate, "v"), *packed,
        scratch=[pltpu.VMEM((2, 2, count, ff), BF16), dma(3), *halves, pltpu.VMEM((2, count, padded), BF16)],
        flops=4 * count * width * ff, mib=14,
    )
    (pair,) = call(
        add_pair, [((count, part + LANES), BF16, "h")], (kept, "v"), (from_low, "v"), (from_high, "v"),
        scratch=[pltpu.VMEM((count, part + LANES), BF16), dma(2)], mib=8,
    )
    returned = exchange(pair.reshape(experts, half, part + LANES)).reshape(count, part + LANES)

    one = pltpu.SemaphoreType.DMA
    shard = ((ff, width), BF16, "h")
    cost = 4 * count * width * ff
    (grad_down,) = call(
        down_grads, [shard],
        (cot, "v"), (mid, "h"), (swap(cot), "h"), (swap(hid), "h"),
        scratch=[
            pltpu.VMEM((2, count, ff), BF16), dma(2), pltpu.VMEM((count, width), BF16), one,
            pltpu.VMEM((ff, width), BF16), one,
        ],
        flops=cost, mib=12,
    )
    grad_gate, grad_up = call(
        row_grads, [shard] * 2,
        (parity, "s"), (sides, "h"), (swap(sides), "h"), (grads, "h"), (swap(theirs), "h"),
        scratch=[
            pltpu.VMEM((2, 2, count, part), BF16), dma(4), pltpu.VMEM((2, count, ff), BF16), dma(4),
            pltpu.VMEM((2, ff, width), BF16), dma(2), pltpu.VMEM((2, count, padded), BF16),
        ],
        flops=2 * cost, mib=18,
    )

    block = (depth // 2, rows + 16, LANES)
    keep, send = call(
        combine, [(block, F32, "v"), (block, BF16, "v")],
        (core, "s"), (table, "v"), (returned, "v"),
        flops=2 * count * rows * part, mib=10,
    )
    turn = lax.axis_index("zh").astype(jnp.int32).reshape(1)
    steps = depth // 2
    parts = call(
        join, [(block[1:], BF16, "v")] * steps,
        (turn, "s"), (keep, "v"), (swap(send), "v"), mib=4,
    )
    sums = [parts[0]] + [shift(parts[k], 2 * k) for k in range(1, steps)]
    grad_tokens, grad_gates = call(
        finish,
        [((rows, LANES), BF16, "w"), ((top_k, rows), F32, "w")],
        (table, "v"), *((v, "v") for v in sums), mib=4,
    )
    return (grad_tokens, grad_gates.T, grad_gate.T[None], grad_up.T[None], grad_down[None])


def solution(mesh):
    devices = mesh.devices.reshape(4, 4, 4, 2, 2)
    inner = jax.sharding.Mesh(devices, (*EP, *Z, "c"))
    ep, tp = EP, (*Z, "c")

    def body(*args):
        return local(16, *args)

    return jax.shard_map(
        body,
        mesh=inner,
        in_specs=(
            P(ep, None),
            P(ep, None),
            P(ep, None),
            P(ep, None),
            P(ep, None, tp),
            P(ep, None, tp),
            P(ep, tp, None),
        ),
        out_specs=(
            P(ep, tp),
            P(ep, None),
            P(ep, None, tp),
            P(ep, None, tp),
            P(ep, tp, None),
        ),
        check_vma=False,
    )
```
